32 devices in a mesh: grp: 2 (over y), sp: 4 (over z), tp: 4 (over x, core).
Axes of the slice: x: 2, y: 2, z: 4, core: 2. Of those that a mesh axis runs over, the one named last changes fastest.
Arguments:
- inputs: bfloat16 [2048, 2048], P(('grp', 'sp'), 'tp'), parts along dimension 0, may hold values from -20 to 20
- norm_gain: bfloat16 [2048], replicated, may hold values from 0.099609375 to 1.8984375
- w_conv_in: bfloat16 [1024, 2048], P('tp'), may hold values from -0.125 to 0.125
- w_conv_gate: bfloat16 [1024, 2048], P('tp'), may hold values from -0.125 to 0.125
- conv_kernel: bfloat16 [31, 1024], P(None, 'tp'), may hold values from -4.3105272 to 4.3105272
- ln_gain: bfloat16 [1024], P('tp'), may hold values from 0.099609375 to 1.8984375
- w_query: bfloat16 [1024, 2048], P('tp'), may hold values from -0.53033009 to 0.53033009
- w_key: bfloat16 [1024, 2048], P('tp'), may hold values from -0.53033009 to 0.53033009
- w_value: bfloat16 [1024, 2048], P('tp'), may hold values from -0.125 to 0.125
- cum_gate: float32 [16, 2048], P('tp', ('grp', 'sp')), parts along dimension 1, may hold values from -1024 to 0, as said below
- w_conv_out: bfloat16 [1024, 2048], P('tp'), may hold values from -0.125 to 0.125
- w_attn_out: bfloat16 [1024, 2048], P('tp'), may hold values from -0.125 to 0.125
Outputs:
- mixed: bfloat16 [2048, 2048], P(('grp', 'sp', 'tp')), parts along dimension 0
- log_total: float32 [16, 2048], P('tp', ('grp', 'sp')), parts along dimension 1
The draws below stay inside these ranges and needn't reach their ends.
There are 2 independent parts, one for each index of `grp`. The reference program is written for one: setup_inputs(seed, part) draws one part's arguments, and reference() takes and returns one part's arrays. A program takes and returns all parts, laid end to end along the dimension named above; an argument that names none is the same for every part. Nothing has to cross between parts.
Inputs may be any that keep to these rules, and one draw needn't show every extreme that they name: cum_gate never rises along positions: entry t is the sum of the head's log forget gates at positions 0 to t.
All inputs are finite; a program needn't handle non-finite values.
Results may differ from the reference program's by a relative error of at most 0.0144.
Values may be sent and summed in bfloat16 or wider, within the bound.
A program may use at most 64 MiB of HBM per device.

```python
import math
import jax
import jax.numpy as jnp
from jax import lax

D = 2048
CONV_CH = 1024
ATTENDER_TOTAL = 16
HEAD_DIM = 64
CONV_WIDTH = 31
TOK_DEV = 256
ATT_W = 1024
SEQUENCE_SPAN = 1024
N_SP = 4
N_TP = 4


def draw_inputs(key, part):
    key_one = jax.random.fold_in(key, 0)
    columns = jnp.exp(jnp.linspace(math.log(0.5), math.log(3.0), D)).astype(jnp.float32)
    raw_draw = jnp.clip(jax.random.normal(key_one, (SEQUENCE_SPAN, D), jnp.float32), -6.0, 6.0)
    return (raw_draw * columns[None, :]).astype(jnp.bfloat16)


def query_key_pair(key):
    query_draw = jnp.clip(jax.random.normal(jax.random.fold_in(key, 11), (ATT_W, D), jnp.float32), -6.0, 6.0) * D ** (-0.5)
    key_draw = 2.0 * jnp.clip(jax.random.normal(jax.random.fold_in(key, 13), (ATT_W, D), jnp.float32), -6.0, 6.0) * D ** (-0.5)
    query_draw = 2.0 * query_draw
    return (query_draw, key_draw)


def draw_w_query(key, part):
    return query_key_pair(key)[0].astype(jnp.bfloat16)


def draw_w_key(key, part):
    return query_key_pair(key)[1].astype(jnp.bfloat16)


def draw_conv_kernel(key, part):
    channels = jnp.exp(jnp.linspace(math.log(0.4), math.log(4.0), CONV_CH)).astype(jnp.float32)
    raw_draw = jnp.clip(jax.random.normal(key, (CONV_WIDTH, CONV_CH), jnp.float32), -6.0, 6.0)
    return (raw_draw * CONV_WIDTH ** (-0.5) * channels[None, :]).astype(jnp.bfloat16)


def draw_cum_gate(key, part):
    derived_seeds = jax.random.split(key, 6)
    head_order = jax.random.permutation(derived_seeds[0], ATTENDER_TOTAL)
    longest_memory_channel = head_order < ATTENDER_TOTAL // 2
    head_rate = jnp.exp(jax.random.uniform(derived_seeds[1], (ATTENDER_TOTAL,), jnp.float32, math.log(0.8), math.log(1.25)))
    base_rate = jnp.where(longest_memory_channel, 0.5 / SEQUENCE_SPAN, 1.0 / 25.0) * head_rate
    block_rate = jnp.exp(jax.random.uniform(derived_seeds[2], (ATTENDER_TOTAL, SEQUENCE_SPAN // TOK_DEV), jnp.float32, math.log(0.5), math.log(2.0)))
    block_rate = jnp.repeat(block_rate, TOK_DEV, axis=1)
    position_rate = jax.random.uniform(derived_seeds[3], (ATTENDER_TOTAL, SEQUENCE_SPAN), jnp.float32, 0.5, 1.5)
    decay_exponent = -base_rate[:, None] * block_rate * position_rate
    contiguous_offset = jax.random.randint(derived_seeds[4], (ATTENDER_TOTAL, 2, 1), 0, SEQUENCE_SPAN)
    contiguous_extent = jax.random.uniform(derived_seeds[5], (ATTENDER_TOTAL, 2, 1), jnp.float32, 0.22, 0.69)
    location_numbers = jnp.arange(SEQUENCE_SPAN, dtype=jnp.int32)
    contiguous_batches = jnp.sum(jnp.where(location_numbers[None, None, :] == contiguous_offset, contiguous_extent, 0.0), axis=1)
    decay_exponent = decay_exponent - jnp.where(longest_memory_channel[:, None], contiguous_batches, 0.0)
    return jnp.cumsum(decay_exponent, axis=1)


def levels(own_key, shape, pieces, least, top_value):
    def one(position, blocks):
        steps = jax.random.uniform(jax.random.fold_in(jax.random.fold_in(own_key, 6), position), (blocks,), jnp.float32, least / len(pieces), top_value / len(pieces))
        return jnp.repeat(jnp.exp(steps), shape[position] // blocks).reshape((-1,) + (1,) * (len(shape) - position - 1))

    level = one(*pieces[0])
    for cut in pieces[1:]:
        level = level * one(*cut)
    return level


def noise(key, shape, spread, most, pieces=(), kind=jnp.bfloat16):
    array = spread * jax.random.normal(key, shape, jnp.float32)
    if pieces:
        array = array * levels(key, shape, pieces, -0.22, 0.18)
    return jnp.clip(array, -most, most).astype(kind)


def setup_inputs(seed: int = 0, part: int = 0) -> dict:
    key_list = jax.random.split(jax.random.key(seed), 13)
    part_splits = jax.random.split(jax.random.fold_in(key_list[12], part), 13)
    return {
        "inputs": draw_inputs(jax.random.fold_in(jax.random.fold_in(key_list[12], part), 71), part),
        "norm_gain": jnp.clip(1.0 + 0.18 * jax.random.normal(key_list[1], (D,), jnp.float32), 0.099609375, 1.8984375).astype(jnp.bfloat16),
        "w_conv_in": noise(key_list[2], (CONV_CH, D), D ** -0.5, 0.125, ((0, 4),)),
        "w_conv_gate": noise(key_list[3], (CONV_CH, D), D ** -0.5, 0.125, ((0, 4),)),
        "conv_kernel": draw_conv_kernel(jax.random.fold_in(key_list[12], 71), part),
        "ln_gain": jnp.clip(1.0 + 0.18 * jax.random.normal(key_list[5], (CONV_CH,), jnp.float32), 0.099609375, 1.8984375).astype(jnp.bfloat16),
        "w_query": draw_w_query(jax.random.fold_in(key_list[12], 71), part),
        "w_key": draw_w_key(jax.random.fold_in(key_list[12], 71), part),
        "w_value": noise(key_list[8], (ATT_W, D), D ** -0.5, 0.125, ((0, 4),)),
        "cum_gate": draw_cum_gate(jax.random.fold_in(jax.random.fold_in(key_list[12], part), 71), part),
        "w_conv_out": noise(key_list[10], (CONV_CH, D), (CONV_CH + ATT_W) ** -0.5, 0.125, ((0, 4),)),
        "w_attn_out": noise(key_list[11], (ATT_W, D), (CONV_CH + ATT_W) ** -0.5, 0.125, ((0, 4),)),
    }


neg_large = -1e+30

def block_terms(q_blk, q_cum, k_blk, v_blk, k_cum, q_first, k_first):
    score_scale = q_blk.shape[2] ** (-0.5)
    scores = jnp.einsum('qhd,khd->hqk', q_blk.astype(jnp.float32), k_blk.astype(jnp.float32)) * score_scale
    scores = scores + q_cum[:, :, None] - k_cum[:, None, :]
    q_pos = q_first + jnp.arange(q_blk.shape[0], dtype=jnp.int32)
    k_pos = k_first + jnp.arange(k_blk.shape[0], dtype=jnp.int32)
    allowed = k_pos[None, :] <= q_pos[:, None]
    scores = jnp.where(allowed[None], scores, -jnp.inf)
    block_top = lax.optimization_barrier(jnp.max(scores, axis=-1))
    weights = jnp.exp(scores - block_top[..., None])
    block_total = lax.optimization_barrier(jnp.sum(weights, axis=-1))
    rounded = lax.optimization_barrier(weights.astype(jnp.bfloat16))
    block_out = jnp.einsum('hqk,khd->hqd', rounded.astype(jnp.float32), v_blk.astype(jnp.float32)).astype(jnp.bfloat16)
    return (block_top, block_total, block_out)

def merge_terms(state, terms):
    top_now, total_now, acc_now = state
    block_top, block_total, block_out = terms
    top_new = jnp.maximum(top_now, block_top)
    keep_old = jnp.exp(top_now - top_new)
    keep_new = jnp.exp(block_top - top_new)
    return (top_new, total_now * keep_old + block_total * keep_new, acc_now * keep_old[..., None] + block_out.astype(jnp.float32) * keep_new[..., None])

def reference(inputs, norm_gain, w_conv_in, w_conv_gate, conv_kernel, ln_gain, w_query, w_key, w_value, cum_gate, w_conv_out, w_attn_out):
    rows_f = inputs.astype(jnp.float32)
    rms = lax.rsqrt(lax.optimization_barrier(jnp.mean(rows_f * rows_f, axis=1, keepdims=True)) + 1e-06)
    scaled = (rows_f * norm_gain.astype(jnp.float32)[None, :]).astype(jnp.bfloat16)

    def project(weight):
        return lax.dot_general(scaled, weight, (((1,), (1,)), ((), ())), preferred_element_type=jnp.float32) * rms
    conv_in = project(w_conv_in)
    conv_gate = project(w_conv_gate)
    glu = (conv_in * jax.nn.sigmoid(conv_gate)).astype(jnp.bfloat16)
    padded = jnp.concatenate([jnp.zeros((CONV_WIDTH - 1, CONV_CH), jnp.bfloat16), glu], axis=0)
    kernel = conv_kernel.astype(jnp.float32)
    conv_sum = jnp.zeros((SEQUENCE_SPAN, CONV_CH), jnp.float32)
    for tap_idx in range(CONV_WIDTH):
        conv_sum = conv_sum + padded[tap_idx:tap_idx + SEQUENCE_SPAN].astype(jnp.float32) * kernel[tap_idx][None, :]
    chan_mean = lax.optimization_barrier(jnp.mean(conv_sum, axis=1, keepdims=True))
    chan_var = lax.optimization_barrier(jnp.mean(conv_sum * conv_sum, axis=1, keepdims=True)) - chan_mean * chan_mean
    normed = (conv_sum - chan_mean) * lax.rsqrt(chan_var + 1e-05) * ln_gain.astype(jnp.float32)[None, :]
    conv_out = jax.nn.silu(normed).astype(jnp.bfloat16)
    query = project(w_query).astype(jnp.bfloat16).reshape(N_SP, TOK_DEV, ATTENDER_TOTAL, HEAD_DIM)
    key_rows = project(w_key).astype(jnp.bfloat16).reshape(N_SP, TOK_DEV, ATTENDER_TOTAL, HEAD_DIM)
    value = project(w_value).astype(jnp.bfloat16).reshape(N_SP, TOK_DEV, ATTENDER_TOTAL, HEAD_DIM)
    cum_blocks = cum_gate.reshape(ATTENDER_TOTAL, N_SP, TOK_DEV).transpose(1, 0, 2)

    def one_query_block(query_idx):
        q_blk = query[query_idx]
        q_cum = cum_blocks[query_idx]

        def visit(key_idx, state):
            terms = block_terms(q_blk, q_cum, key_rows[key_idx], value[key_idx], cum_blocks[key_idx], query_idx * TOK_DEV, key_idx * TOK_DEV)
            return merge_terms(state, terms)
        start_state = (jnp.full((ATTENDER_TOTAL, TOK_DEV), neg_large, jnp.float32), jnp.zeros((ATTENDER_TOTAL, TOK_DEV), jnp.float32), jnp.zeros((ATTENDER_TOTAL, TOK_DEV, HEAD_DIM), jnp.float32))
        top_all, total_all, acc_all = lax.fori_loop(0, query_idx + 1, visit, start_state)
        result = (acc_all / total_all[..., None]).transpose(1, 0, 2).reshape(TOK_DEV, ATT_W).astype(jnp.bfloat16)
        return (result, top_all + jnp.log(total_all))
    attn_blocks, log_blocks = lax.map(one_query_block, jnp.arange(N_SP, dtype=jnp.int32))
    attn_out = attn_blocks.reshape(SEQUENCE_SPAN, ATT_W)
    log_total = log_blocks.transpose(1, 0, 2).reshape(ATTENDER_TOTAL, SEQUENCE_SPAN)
    chan_group = CONV_CH // N_TP
    head_group = ATT_W // N_TP
    mixed = jnp.zeros((SEQUENCE_SPAN, D), jnp.float32)
    for group_idx in range(N_TP):
        part = jnp.dot(conv_out[:, group_idx * chan_group:(group_idx + 1) * chan_group], w_conv_out[group_idx * chan_group:(group_idx + 1) * chan_group], preferred_element_type=jnp.float32)
        part = part + jnp.dot(attn_out[:, group_idx * head_group:(group_idx + 1) * head_group], w_attn_out[group_idx * head_group:(group_idx + 1) * head_group], preferred_element_type=jnp.float32)
        part_round = lax.optimization_barrier(part.astype(jnp.bfloat16))
        mixed = mixed + part_round.astype(jnp.float32)
    return (mixed.astype(jnp.bfloat16), log_total)
```

```python
import functools
import jax
import jax.numpy as jnp
from jax import lax
from jax.experimental import pallas as pl
from jax.experimental.pallas import tpu as pltpu
from jax.sharding import PartitionSpec as P

D = 2048
CONV_CH = 1024
HEADS = 16


neg_large = -1e30


def passed_along(block, axis, distance):
    devices = range(lax.axis_size(axis))
    route = [(i - distance, i) for i in devices if i - distance in devices]
    return lax.ppermute(block, axis, route)


def block_terms(q_blk, q_cum, k_blk, v_blk, k_cum, q_first, k_first):
    score_scale = q_blk.shape[2] ** (-0.5)
    scores = (
        jnp.einsum("qhd,khd->hqk", q_blk, k_blk, preferred_element_type=jnp.float32) * score_scale
    )
    scores = scores + q_cum[:, :, None] - k_cum[:, None, :]
    q_pos = q_first + jnp.arange(q_blk.shape[0], dtype=jnp.int32)
    k_pos = k_first + jnp.arange(k_blk.shape[0], dtype=jnp.int32)
    allowed = k_pos[None, :] <= q_pos[:, None]
    scores = jnp.where(allowed[None], scores, -jnp.inf)
    block_top = jnp.max(scores, axis=-1)
    weights = jnp.exp(scores - block_top[..., None])
    block_total = jnp.sum(weights, axis=-1)
    block_out = jnp.einsum(
        "hqk,khd->hqd", weights.astype(jnp.bfloat16), v_blk, preferred_element_type=jnp.float32
    ).astype(jnp.bfloat16)
    return (block_top, block_total, block_out)


def merge_terms(state, terms):
    top_now, total_now, acc_now = state
    block_top, block_total, block_out = terms
    top_new = jnp.maximum(top_now, block_top)
    keep_old = jnp.exp(top_now - top_new)
    keep_new = jnp.exp(block_top - top_new)
    return (
        top_new,
        total_now * keep_old + block_total * keep_new,
        acc_now * keep_old[..., None] + block_out.astype(jnp.float32) * keep_new[..., None],
    )


def local(
    inputs,
    norm_gain,
    w_conv_in,
    w_conv_gate,
    conv_kernel,
    ln_gain,
    w_query,
    w_key,
    w_value,
    cum_gate,
    w_conv_out,
    w_attn_out,
):
    rows_here = inputs.shape[0]
    conv_width = w_conv_in.shape[0]
    attn_width = w_query.shape[0]
    heads_here = cum_gate.shape[0]
    head_dim = attn_width // heads_here
    taps_count = conv_kernel.shape[0]
    w_all = jnp.concatenate([w_conv_in, w_conv_gate, w_query, w_key, w_value], axis=0)
    gain_all = norm_gain.astype(jnp.float32)
    contract_dims = (((1,), (1,)), ((), ()))
    piece_f = lax.all_gather(inputs, "tp", axis=1, tiled=True).astype(jnp.float32)
    scaled_piece = (piece_f * gain_all[None, :]).astype(jnp.bfloat16)
    raw_proj = lax.dot_general(
        scaled_piece, w_all, contract_dims, preferred_element_type=jnp.float32
    )
    squares = jnp.sum(piece_f * piece_f, axis=1)
    rms = lax.rsqrt(squares / D + 1e-06)[:, None]
    proj = raw_proj * rms
    conv_in = proj[:, :conv_width]
    conv_gate = proj[:, conv_width : 2 * conv_width]
    query = proj[:, 2 * conv_width : 2 * conv_width + attn_width].astype(jnp.bfloat16)
    key_rows = proj[:, 2 * conv_width + attn_width : 2 * conv_width + 2 * attn_width].astype(
        jnp.bfloat16
    )
    value = proj[:, 2 * conv_width + 2 * attn_width :].astype(jnp.bfloat16)
    glu = (conv_in * jax.nn.sigmoid(conv_gate)).astype(jnp.bfloat16)
    rim_rows = passed_along(glu[rows_here - (taps_count - 1) :], "sp", 1)
    extended = jnp.concatenate([rim_rows, glu], axis=0)
    kernel = conv_kernel.astype(jnp.float32)
    conv_sum = jnp.zeros((rows_here, conv_width), jnp.float32)
    for tap_idx in range(taps_count):
        conv_sum = (
            conv_sum
            + extended[tap_idx : tap_idx + rows_here].astype(jnp.float32) * kernel[tap_idx][None, :]
        )
    chan_first, chan_second = lax.psum(
        (jnp.sum(conv_sum, axis=1), jnp.sum(conv_sum * conv_sum, axis=1)), "tp"
    )
    chan_mean = (chan_first / CONV_CH)[:, None]
    chan_var = (chan_second / CONV_CH)[:, None] - chan_mean * chan_mean
    normed = (
        (conv_sum - chan_mean) * lax.rsqrt(chan_var + 1e-05) * ln_gain.astype(jnp.float32)[None, :]
    )
    conv_out = jax.nn.silu(normed).astype(jnp.bfloat16)
    q_heads = query.reshape(rows_here, heads_here, head_dim)
    cum_all = lax.all_gather(cum_gate.T, "sp", axis=0, tiled=True)
    own_first = lax.axis_index("sp") * rows_here
    start_state = (
        jnp.full((heads_here, rows_here), neg_large, jnp.float32),
        jnp.zeros((heads_here, rows_here), jnp.float32),
        jnp.zeros((heads_here, rows_here, head_dim), jnp.float32),
    )
    state = start_state
    k_piece = lax.all_gather(key_rows, "sp", axis=0, tiled=True)
    v_piece = lax.all_gather(value, "sp", axis=0, tiled=True)
    block_count = k_piece.shape[0] // rows_here
    k_split = k_piece.reshape(block_count, rows_here, heads_here, head_dim)
    v_split = v_piece.reshape(block_count, rows_here, heads_here, head_dim)

    def visit(carry, item):
        k_blk, v_blk, block_idx = item
        k_first = block_idx * rows_here
        k_cum = lax.dynamic_slice_in_dim(cum_all, k_first, rows_here, 0).T

        def take_block(inner):
            return merge_terms(
                inner, block_terms(q_heads, cum_gate, k_blk, v_blk, k_cum, own_first, k_first)
            )

        def skip_block(inner):
            return inner

        return (lax.cond(k_first <= own_first, take_block, skip_block, carry), None)

    state, unused = lax.scan(
        visit, state, (k_split, v_split, jnp.arange(block_count, dtype=jnp.int32))
    )
    top_all, total_all, acc_all = state
    attn_out = (
        (acc_all / total_all[..., None])
        .transpose(1, 0, 2)
        .reshape(rows_here, attn_width)
        .astype(jnp.bfloat16)
    )
    log_total = top_all + jnp.log(total_all)
    mixed = lax.psum_scatter(
        (
            jnp.dot(conv_out, w_conv_out, preferred_element_type=jnp.float32)
            + jnp.dot(attn_out, w_attn_out, preferred_element_type=jnp.float32)
        ).astype(jnp.bfloat16),
        "tp",
        scatter_dimension=0,
        tiled=True,
    )
    return (mixed, log_total)


AG_CHUNKS = 4
OUT_CHUNKS = 4
MESH = pl.DeviceIdType.MESH
NT = (((1,), (1,)), ((), ()))


def fused_kernel(
    n_sp,
    n_tp,
    x_hbm,
    gain_ref,
    wci_hbm,
    wcg_hbm,
    ck_ref,
    lng_ref,
    wq_hbm,
    wk_hbm,
    wv_hbm,
    cum_ref,
    wco_hbm,
    wao_hbm,
    out_ref,
    log_ref,
    xg,
    xs,
    wbuf,
    wco,
    wao,
    acc,
    ss,
    zsend,
    zrecv,
    q_s,
    k_s,
    v_s,
    cum_recv,
    ext,
    glu_s,
    halo,
    csum,
    st_send,
    st_recv,
    cpart,
    ret_send,
    ret_recv,
    att_s,
    lse_send,
    lse_recv,
    d_send,
    d_recv,
    x_send,
    x_recv,
    own_part,
    wsem,
    owsem,
    xsem,
    ag_send,
    ag_recv,
    zs_sem,
    zr_sem,
    cs_sem,
    cr_sem,
    hs_sem,
    hr_sem,
    ss_sem,
    sr_sem,
    rs_sem,
    rr_sem,
    ls_sem,
    lr_sem,
    ds_sem,
    dr_sem,
    xs_sem,
    xr_sem,
):
    f32, bf16 = jnp.float32, jnp.bfloat16
    z = lax.axis_index("sp")
    me = lax.axis_index("tp")
    chip, core = me // 2, me % 2
    chips = n_tp // 2
    rows, width = x_hbm.shape
    conv_w = wci_hbm.shape[0]
    attn_w = wq_hbm.shape[0]
    heads = n_sp
    hd = attn_w // heads
    d_all = wci_hbm.shape[1]
    partner = chip * 2 + 1 - core

    def remote(src, dst, s, r, dev):
        return pltpu.make_async_remote_copy(
            src_ref=src, dst_ref=dst, send_sem=s, recv_sem=r, device_id=dev, device_id_type=MESH
        )

    def same_core(dist):
        return lax.rem(chip + dist, chips) * 2 + core

    def other_core(dist):
        return lax.rem(chip + dist, chips) * 2 + 1 - core

    def piece_owner(rel):
        return same_core(rel // 2) if rel % 2 == 0 else other_core(rel // 2)

    def piece_source(rel):
        back = chips - rel // 2
        return same_core(back) if rel % 2 == 0 else other_core(back)

    barrier = pltpu.get_barrier_semaphore()
    for rel in range(1, n_tp):
        pl.semaphore_signal(
            barrier, inc=1, device_id={"tp": piece_owner(rel)}, device_id_type=MESH
        )
    for dist in range(1, n_sp):
        pl.semaphore_signal(
            barrier, inc=1, device_id={"sp": lax.rem(z + dist, n_sp)}, device_id_type=MESH
        )

    own_copy = pltpu.make_async_copy(x_hbm, xg.at[0], xsem)
    own_copy.start()
    loads = []
    for h in range(heads):
        loads.append((wq_hbm.at[pl.ds(h * hd, hd)], wbuf.at[pl.ds(2 * h * hd, hd)]))
        loads.append((wk_hbm.at[pl.ds(h * hd, hd)], wbuf.at[pl.ds((2 * h + 1) * hd, hd)]))
    loads.append((wv_hbm, wbuf.at[pl.ds(2 * attn_w, attn_w)]))
    qkv_loads = len(loads)
    qkv_w = 3 * attn_w
    loads.append((wci_hbm, wbuf.at[pl.ds(qkv_w, conv_w)]))
    loads.append((wcg_hbm, wbuf.at[pl.ds(qkv_w + conv_w, conv_w)]))
    wcopies = [pltpu.make_async_copy(a, b, wsem.at[i]) for i, (a, b) in enumerate(loads)]
    wco_copy = pltpu.make_async_copy(wco_hbm, wco, owsem.at[0])
    wao_copy = pltpu.make_async_copy(wao_hbm, wao, owsem.at[1])
    for c in wcopies:
        c.start()
    wco_copy.start()
    wao_copy.start()

    pl.semaphore_wait(barrier, n_tp - 1 + n_sp - 1)

    rc = rows // AG_CHUNKS

    def ag_copy(rel, kind, c):
        r = pl.ds(c * rc, rc)
        if kind == "own":
            return remote(
                x_hbm.at[r], xg.at[rel, r], ag_send.at[rel, c], ag_recv.at[rel, c],
                {"tp": piece_owner(rel)},
            )
        return remote(
            xg.at[rel - 1, r], xg.at[rel, r], ag_send.at[rel, c], ag_recv.at[rel, c],
            {"tp": partner},
        )

    ag = {}
    for c in range(AG_CHUNKS):
        for dist in range(1, chips):
            ag[2 * dist, c] = ag_copy(2 * dist, "own", c)
            ag[2 * dist, c].start()
    for c in range(AG_CHUNKS):
        ag[1, c] = ag_copy(1, "own", c)
        ag[1, c].start()
    cums = []
    for dist in range(1, n_sp):
        cp = remote(
            cum_ref, cum_recv.at[z], cs_sem.at[dist], cr_sem.at[dist],
            {"sp": lax.rem(z + dist, n_sp)},
        )
        cp.start()
        cums.append(cp)
    cum_recv[z] = cum_ref[...]

    def prepare(rel, c0, n):
        r = pl.ds(c0, n)
        owner = piece_source(rel)
        raw = xg[rel, r].astype(f32)
        g = gain_ref[:, pl.ds(pl.multiple_of(owner * width, width), width)].astype(f32)
        xs[rel, r] = (raw * g).astype(bf16)
        return jnp.sum(raw * raw, axis=1, keepdims=True)

    def wcols(rel, first, n):
        owner = piece_source(rel)
        return wbuf[pl.ds(first, n), pl.ds(pl.multiple_of(owner * width, width), width)]

    own_copy.wait()
    ss[...] = prepare(0, 0, rows)
    for c in wcopies[:qkv_loads]:
        c.wait()
    acc[:, :qkv_w] = lax.dot_general(xs[0], wcols(0, 0, qkv_w), NT, preferred_element_type=f32)
    for c in wcopies[qkv_loads:]:
        c.wait()
    acc[:, qkv_w:] = lax.dot_general(
        xs[0], wcols(0, qkv_w, 2 * conv_w), NT, preferred_element_type=f32
    )
    for c in range(AG_CHUNKS):
        ag[1, c].wait_recv()
    ss[...] += prepare(1, 0, rows)
    acc[...] += lax.dot_general(
        xs[1], wcols(1, 0, qkv_w + 2 * conv_w), NT, preferred_element_type=f32
    )

    half = rc // 2
    for c in range(AG_CHUNKS):
        r = pl.ds(c * rc, rc)
        for dist in range(1, chips):
            ag[2 * dist, c].wait_recv()
            ag[2 * dist + 1, c] = ag_copy(2 * dist + 1, "relay", c)
            ag[2 * dist + 1, c].start()
        total = acc[r, :qkv_w]
        sq = ss[r]
        for dist in range(1, chips):
            for rel in (2 * dist, 2 * dist + 1):
                if rel % 2 == 1:
                    ag[rel, c].wait_recv()
                sq = sq + prepare(rel, c * rc, rc)
                total = total + lax.dot_general(
                    xs[rel, r], wcols(rel, 0, qkv_w), NT, preferred_element_type=f32
                )
        rms = lax.rsqrt(sq / d_all + 1e-06)
        ss[r] = rms
        total = total * rms
        for h in range(heads):
            zsend[h, c, :rc] = total[:, 2 * h * hd : 2 * (h + 1) * hd].astype(bf16)
            v_h = total[:, 2 * attn_w + h * hd : 2 * attn_w + (h + 1) * hd]
            zsend[h, c, rc:] = jnp.concatenate([v_h[:half], v_h[half:]], axis=1).astype(bf16)
        for dist in range(n_sp - 1, 0, -1):
            to = lax.rem(z + dist, n_sp)
            remote(
                zsend.at[to, c], zrecv.at[z, c], zs_sem.at[dist, c], zr_sem.at[dist, c], {"sp": to}
            ).start()
        zrecv[z, c] = zsend[z, c]

    pre = acc[:, qkv_w:]
    for rel in range(2, n_tp):
        pre = pre + lax.dot_general(
            xs[rel], wcols(rel, qkv_w, 2 * conv_w), NT, preferred_element_type=f32
        )
    pre = pre * ss[...]
    glu = (pre[:, :conv_w] * jax.nn.sigmoid(pre[:, conv_w:])).astype(bf16)
    glu_s[...] = glu
    taps = ck_ref.shape[0]
    rim = halo.shape[0]
    ext[rim:, :] = glu.astype(f32)
    halo_copy = remote(
        glu_s.at[pl.ds(rows - rim, rim)], halo, hs_sem, hr_sem, {"sp": lax.rem(z + 1, n_sp)}
    )

    @pl.when(z < n_sp - 1)
    def _():
        halo_copy.start()

    @pl.when(z == 0)
    def _():
        halo[...] = jnp.zeros_like(halo)

    @pl.when(z > 0)
    def _():
        halo_copy.wait_recv()

    ext[:rim, :] = halo[...].astype(f32)

    blk = 64

    def conv_block(b, carry):
        first = pl.multiple_of(b * blk, blk)
        block = ext[pl.ds(first, blk + rim), :]
        tot = jnp.zeros((blk, conv_w), f32)
        for j in range(taps):
            off = rim - (taps - 1) + j
            tot = tot + block[off : off + blk] * ck_ref[j : j + 1, :].astype(f32)
        csum[pl.ds(first, blk), :] = tot
        return carry

    lax.fori_loop(0, rows // blk, conv_block, 0)
    cs = csum[...]
    first = jnp.sum(cs, axis=1, keepdims=True)
    second = jnp.sum(cs * cs, axis=1, keepdims=True)
    lane = lax.broadcasted_iota(jnp.int32, (rows, 128), 1)
    both = jnp.where(lane == 0, first, second)
    st_send[...] = both.T[: st_send.shape[0]]
    stats = []
    for rel in range(1, n_tp):
        cp = remote(
            st_send, st_recv.at[rel - 1], ss_sem.at[rel], sr_sem.at[rel], {"tp": piece_owner(rel)}
        )
        cp.start()
        stats.append(cp)
    tot = st_send[...]
    for rel in range(1, n_tp):
        stats[rel - 1].wait_recv()
        tot = tot + st_recv[rel - 1]
    wide = jnp.concatenate([tot] * (128 // tot.shape[0]), axis=0).T
    mean = wide[:, 0:1] / CONV_CH
    var = wide[:, 1:2] / CONV_CH - mean * mean
    normed = (csum[...] - mean) * lax.rsqrt(var + 1e-05) * lng_ref[...].astype(f32)
    conv_out = (normed / (1.0 + jnp.exp(-normed))).astype(bf16)
    wco_copy.wait()
    cpart[...] = jnp.dot(conv_out, wco[...], preferred_element_type=f32)

    for cp in cums:
        cp.wait_recv()
    for dist in range(n_sp - 1, 0, -1):
        for c in range(AG_CHUNKS):
            src = lax.rem(z + dist, n_sp)
            remote(
                zsend.at[src, c],
                zrecv.at[src, c],
                zs_sem.at[n_sp - dist, c],
                zr_sem.at[n_sp - dist, c],
                {"sp": src},
            ).wait_recv()
    for s in range(n_sp):
        for c in range(AG_CHUNKS):
            r0 = s * rows + c * rc
            tile = zrecv[s, c, :rc].astype(f32)
            q_s[pl.ds(r0, rc)] = tile[:, :hd].astype(bf16)
            k_s[pl.ds(r0, rc)] = tile[:, hd:].astype(bf16)
            vt = zrecv[s, c, rc:].astype(f32)
            v_s[pl.ds(r0, half)] = vt[:, :hd].astype(bf16)
            v_s[pl.ds(r0 + half, half)] = vt[:, hd:].astype(bf16)
    scale = hd ** (-0.5)
    hrows = rows // 2
    for i in range(n_sp - 1, -1, -1):
        keys = (i + 1) * rows
        q = q_s[pl.ds(i * rows, rows)]
        cum_k = jnp.concatenate([cum_recv[s, pl.ds(z, 1)] for s in range(i + 1)], axis=1)
        sc = lax.dot_general(q, k_s[:keys], NT, preferred_element_type=f32) * scale - cum_k
        q_pos = i * rows + lax.broadcasted_iota(jnp.int32, (rows, keys), 0)
        k_pos = lax.broadcasted_iota(jnp.int32, (rows, keys), 1)
        sc = jnp.where(k_pos <= q_pos, sc, -jnp.inf)
        top = jnp.max(sc, axis=1, keepdims=True)
        p = jnp.exp(sc - top)
        tot = jnp.sum(p, axis=1, keepdims=True)
        o = jnp.dot(p.astype(bf16), v_s[:keys], preferred_element_type=f32) / tot
        ret_send[i] = jnp.concatenate([o[:hrows], o[hrows:]], axis=1).astype(bf16)
        lse = jnp.broadcast_to(top + jnp.log(tot), (rows, 128)).T[:8]
        lse_send[i] = lse + cum_recv[i, pl.ds(z, 1)]

        @pl.when(z != i)
        def _():
            remote(
                ret_send.at[i], ret_recv.at[z], rs_sem.at[i], rr_sem.at[z], {"sp": i}
            ).start()
            remote(
                lse_send.at[i], lse_recv.at[z], ls_sem.at[i], lr_sem.at[z], {"sp": i}
            ).start()

        @pl.when(z == i)
        def _():
            ret_recv[i] = ret_send[i]
            lse_recv[i] = lse_send[i]

    for h in range(n_sp):

        @pl.when(z != h)
        def _():
            remote(
                ret_send.at[h], ret_recv.at[h], rs_sem.at[h], rr_sem.at[h], {"sp": h}
            ).wait_recv()
            remote(
                lse_send.at[h], lse_recv.at[h], ls_sem.at[h], lr_sem.at[h], {"sp": h}
            ).wait_recv()

    got = [ret_recv[h].astype(f32) for h in range(n_sp)]
    att_s[:hrows] = jnp.concatenate([g[:, :hd] for g in got], axis=1).astype(bf16)
    att_s[hrows:] = jnp.concatenate([g[:, hd:] for g in got], axis=1).astype(bf16)
    for h in range(n_sp):
        log_ref[pl.ds(h, 1), :] = lse_recv[h, 0:1, :]
    wao_copy.wait()

    own_rows = rows // n_tp
    cw = d_all // OUT_CHUNKS

    def part_of(owner, n):
        r = pl.ds(pl.multiple_of(owner * own_rows, own_rows), own_rows)
        cols = slice(n * cw, (n + 1) * cw)
        return cpart[r, cols] + jnp.dot(att_s[r, :], wao[:, cols], preferred_element_type=f32)

    order = [dist for dist in range(1, chips)] + [0]
    d2d = {}
    for dist in order:
        for n in range(OUT_CHUNKS):
            d_send[dist, n] = part_of(other_core(dist), n).astype(bf16)
            d2d[dist, n] = remote(
                d_send.at[dist, n],
                d_recv.at[dist, n],
                ds_sem.at[dist, n],
                dr_sem.at[dist, n],
                {"tp": partner},
            )
            d2d[dist, n].start()
    xc = {}
    for dist in range(1, chips):
        for n in range(OUT_CHUNKS):
            mine = part_of(same_core(dist), n)
            d2d[dist, n].wait_recv()
            x_send[dist - 1, n] = (mine + d_recv[dist, n].astype(f32)).astype(bf16)
            xc[dist, n] = remote(
                x_send.at[dist - 1, n],
                x_recv.at[dist - 1, n],
                xs_sem.at[dist - 1, n],
                xr_sem.at[dist - 1, n],
                {"tp": same_core(dist)},
            )
            xc[dist, n].start()
    for n in range(OUT_CHUNKS):
        mine = part_of(me, n)
        d2d[0, n].wait_recv()
        own_part[n] = mine + d_recv[0, n].astype(f32)
    for n in range(OUT_CHUNKS):
        tot = own_part[n]
        for dist in range(1, chips):
            xc[dist, n].wait_recv()
            tot = tot + x_recv[dist - 1, n].astype(f32)
        out_ref[:, n * cw : (n + 1) * cw] = tot.astype(bf16)

    for cp in list(ag.values()) + cums + stats + list(d2d.values()) + list(xc.values()):
        cp.wait_send()

    @pl.when(z < n_sp - 1)
    def _():
        halo_copy.wait_send()

    for dist in range(1, n_sp):
        to = lax.rem(z + dist, n_sp)
        for c in range(AG_CHUNKS):
            remote(
                zsend.at[to, c], zrecv.at[z, c], zs_sem.at[dist, c], zr_sem.at[dist, c], {"sp": to}
            ).wait_send()
    for i in range(n_sp):

        @pl.when(z != i)
        def _():
            remote(
                ret_send.at[i], ret_recv.at[z], rs_sem.at[i], rr_sem.at[z], {"sp": i}
            ).wait_send()
            remote(
                lse_send.at[i], lse_recv.at[z], ls_sem.at[i], lr_sem.at[z], {"sp": i}
            ).wait_send()


def fused_local(
    n_sp,
    n_tp,
    inputs,
    norm_gain,
    w_conv_in,
    w_conv_gate,
    conv_kernel,
    ln_gain,
    w_query,
    w_key,
    w_value,
    cum_gate,
    w_conv_out,
    w_attn_out,
):
    f32, bf16 = jnp.float32, jnp.bfloat16
    rows, width = inputs.shape
    conv_w, d_all = w_conv_in.shape
    attn_w = w_query.shape[0]
    heads = cum_gate.shape[0]
    hd = attn_w // heads
    chips = n_tp // 2
    own_rows = rows // n_tp
    rc = rows // AG_CHUNKS
    rim = -(-(conv_kernel.shape[0] - 1) // 16) * 16
    cw = d_all // OUT_CHUNKS
    all_w = 3 * attn_w + 2 * conv_w
    dma = pltpu.SemaphoreType.DMA
    scratch = [
        pltpu.VMEM((n_tp, rows, width), bf16),
        pltpu.VMEM((n_tp, rows, width), bf16),
        pltpu.VMEM((all_w, d_all), bf16),
        pltpu.VMEM((conv_w, d_all), bf16),
        pltpu.VMEM((attn_w, d_all), bf16),
        pltpu.VMEM((rows, all_w), f32),
        pltpu.VMEM((rows, 1), f32),
        pltpu.VMEM((n_sp, AG_CHUNKS, rc + rc // 2, 2 * hd), bf16),
        pltpu.VMEM((n_sp, AG_CHUNKS, rc + rc // 2, 2 * hd), bf16),
        pltpu.VMEM((n_sp * rows, hd), bf16),
        pltpu.VMEM((n_sp * rows, hd), bf16),
        pltpu.VMEM((n_sp * rows, hd), bf16),
        pltpu.VMEM((n_sp, heads, rows), f32),
        pltpu.VMEM((rows + rim, conv_w), f32),
        pltpu.VMEM((rows, conv_w), bf16),
        pltpu.VMEM((rim, conv_w), bf16),
        pltpu.VMEM((rows, conv_w), f32),
        pltpu.VMEM((8, rows), f32),
        pltpu.VMEM((n_tp - 1, 8, rows), f32),
        pltpu.VMEM((rows, d_all), f32),
        pltpu.VMEM((n_sp, rows // 2, 2 * hd), bf16),
        pltpu.VMEM((n_sp, rows // 2, 2 * hd), bf16),
        pltpu.VMEM((rows, attn_w), bf16),
        pltpu.VMEM((n_sp, 8, rows), f32),
        pltpu.VMEM((n_sp, 8, rows), f32),
        pltpu.VMEM((chips, OUT_CHUNKS, own_rows, cw), bf16),
        pltpu.VMEM((chips, OUT_CHUNKS, own_rows, cw), bf16),
        pltpu.VMEM((chips - 1, OUT_CHUNKS, own_rows, cw), bf16),
        pltpu.VMEM((chips - 1, OUT_CHUNKS, own_rows, cw), bf16),
        pltpu.VMEM((OUT_CHUNKS, own_rows, cw), f32),
        dma((2 * heads + 3,)),
        dma((2,)),
        dma,
        dma((n_tp, AG_CHUNKS)),
        dma((n_tp, AG_CHUNKS)),
        dma((n_sp, AG_CHUNKS)),
        dma((n_sp, AG_CHUNKS)),
        dma((n_sp,)),
        dma((n_sp,)),
        dma,
        dma,
        dma((n_tp,)),
        dma((n_tp,)),
        dma((n_sp,)),
        dma((n_sp,)),
        dma((n_sp,)),
        dma((n_sp,)),
        dma((chips, OUT_CHUNKS)),
        dma((chips, OUT_CHUNKS)),
        dma((chips - 1, OUT_CHUNKS)),
        dma((chips - 1, OUT_CHUNKS)),
    ]
    far = pl.BlockSpec(memory_space=pl.ANY)
    near = pl.BlockSpec(memory_space=pltpu.VMEM)
    mixed, log_total = pl.pallas_call(
        functools.partial(fused_kernel, n_sp, n_tp),
        out_shape=(
            jax.ShapeDtypeStruct((own_rows, d_all), bf16),
            jax.ShapeDtypeStruct((heads, rows), f32),
        ),
        in_specs=[far, near, far, far, near, near, far, far, far, near, far, far],
        out_specs=(near, near),
        scratch_shapes=scratch,
        compiler_params=pltpu.CompilerParams(
            collective_id=0, has_side_effects=True, vmem_limit_bytes=60 * 1024 * 1024
        ),
    )(
        inputs,
        norm_gain.reshape(1, -1),
        w_conv_in,
        w_conv_gate,
        conv_kernel,
        ln_gain.reshape(1, -1),
        w_query,
        w_key,
        w_value,
        cum_gate,
        w_conv_out,
        w_attn_out,
    )
    return (mixed, log_total)


def solution(mesh):
    in_specs = (
        P(("grp", "sp"), "tp"),
        P(),
        P("tp", None),
        P("tp", None),
        P(None, "tp"),
        P("tp"),
        P("tp", None),
        P("tp", None),
        P("tp", None),
        P("tp", ("grp", "sp")),
        P("tp", None),
        P("tp", None),
    )
    out_specs = (P(("grp", "sp", "tp"), None), P("tp", ("grp", "sp")))
    heads_here = HEADS // mesh.shape["tp"]
    fits = heads_here == mesh.shape["sp"] and mesh.shape["tp"] % 2 == 0
    body = functools.partial(fused_local, mesh.shape["sp"], mesh.shape["tp"]) if fits else local
    return jax.shard_map(body, mesh=mesh, in_specs=in_specs, out_specs=out_specs, check_vma=False)
```

```python
import functools
import jax
import jax.numpy as jnp
from jax import lax
from jax.experimental import pallas as pl
from jax.experimental.pallas import tpu as pltpu
from jax.sharding import PartitionSpec as P

D = 2048
CONV_CH = 1024
HEADS = 16


neg_large = -1e30


def passed_along(block, axis, distance):
    devices = range(lax.axis_size(axis))
    route = [(i - distance, i) for i in devices if i - distance in devices]
    return lax.ppermute(block, axis, route)


def block_terms(q_blk, q_cum, k_blk, v_blk, k_cum, q_first, k_first):
    score_scale = q_blk.shape[2] ** (-0.5)
    scores = (
        jnp.einsum("qhd,khd->hqk", q_blk, k_blk, preferred_element_type=jnp.float32) * score_scale
    )
    scores = scores + q_cum[:, :, None] - k_cum[:, None, :]
    q_pos = q_first + jnp.arange(q_blk.shape[0], dtype=jnp.int32)
    k_pos = k_first + jnp.arange(k_blk.shape[0], dtype=jnp.int32)
    allowed = k_pos[None, :] <= q_pos[:, None]
    scores = jnp.where(allowed[None], scores, -jnp.inf)
    block_top = jnp.max(scores, axis=-1)
    weights = jnp.exp(scores - block_top[..., None])
    block_total = jnp.sum(weights, axis=-1)
    block_out = jnp.einsum(
        "hqk,khd->hqd", weights.astype(jnp.bfloat16), v_blk, preferred_element_type=jnp.float32
    ).astype(jnp.bfloat16)
    return (block_top, block_total, block_out)


def merge_terms(state, terms):
    top_now, total_now, acc_now = state
    block_top, block_total, block_out = terms
    top_new = jnp.maximum(top_now, block_top)
    keep_old = jnp.exp(top_now - top_new)
    keep_new = jnp.exp(block_top - top_new)
    return (
        top_new,
        total_now * keep_old + block_total * keep_new,
        acc_now * keep_old[..., None] + block_out.astype(jnp.float32) * keep_new[..., None],
    )


def local(
    inputs,
    norm_gain,
    w_conv_in,
    w_conv_gate,
    conv_kernel,
    ln_gain,
    w_query,
    w_key,
    w_value,
    cum_gate,
    w_conv_out,
    w_attn_out,
):
    rows_here = inputs.shape[0]
    conv_width = w_conv_in.shape[0]
    attn_width = w_query.shape[0]
    heads_here = cum_gate.shape[0]
    head_dim = attn_width // heads_here
    taps_count = conv_kernel.shape[0]
    w_all = jnp.concatenate([w_conv_in, w_conv_gate, w_query, w_key, w_value], axis=0)
    gain_all = norm_gain.astype(jnp.float32)
    contract_dims = (((1,), (1,)), ((), ()))
    piece_f = lax.all_gather(inputs, "tp", axis=1, tiled=True).astype(jnp.float32)
    scaled_piece = (piece_f * gain_all[None, :]).astype(jnp.bfloat16)
    raw_proj = lax.dot_general(
        scaled_piece, w_all, contract_dims, preferred_element_type=jnp.float32
    )
    squares = jnp.sum(piece_f * piece_f, axis=1)
    rms = lax.rsqrt(squares / D + 1e-06)[:, None]
    proj = raw_proj * rms
    conv_in = proj[:, :conv_width]
    conv_gate = proj[:, conv_width : 2 * conv_width]
    query = proj[:, 2 * conv_width : 2 * conv_width + attn_width].astype(jnp.bfloat16)
    key_rows = proj[:, 2 * conv_width + attn_width : 2 * conv_width + 2 * attn_width].astype(
        jnp.bfloat16
    )
    value = proj[:, 2 * conv_width + 2 * attn_width :].astype(jnp.bfloat16)
    glu = (conv_in * jax.nn.sigmoid(conv_gate)).astype(jnp.bfloat16)
    rim_rows = passed_along(glu[rows_here - (taps_count - 1) :], "sp", 1)
    extended = jnp.concatenate([rim_rows, glu], axis=0)
    kernel = conv_kernel.astype(jnp.float32)
    conv_sum = jnp.zeros((rows_here, conv_width), jnp.float32)
    for tap_idx in range(taps_count):
        conv_sum = (
            conv_sum
            + extended[tap_idx : tap_idx + rows_here].astype(jnp.float32) * kernel[tap_idx][None, :]
        )
    chan_first, chan_second = lax.psum(
        (jnp.sum(conv_sum, axis=1), jnp.sum(conv_sum * conv_sum, axis=1)), "tp"
    )
    chan_mean = (chan_first / CONV_CH)[:, None]
    chan_var = (chan_second / CONV_CH)[:, None] - chan_mean * chan_mean
    normed = (
        (conv_sum - chan_mean) * lax.rsqrt(chan_var + 1e-05) * ln_gain.astype(jnp.float32)[None, :]
    )
    conv_out = jax.nn.silu(normed).astype(jnp.bfloat16)
    q_heads = query.reshape(rows_here, heads_here, head_dim)
    cum_all = lax.all_gather(cum_gate.T, "sp", axis=0, tiled=True)
    own_first = lax.axis_index("sp") * rows_here
    start_state = (
        jnp.full((heads_here, rows_here), neg_large, jnp.float32),
        jnp.zeros((heads_here, rows_here), jnp.float32),
        jnp.zeros((heads_here, rows_here, head_dim), jnp.float32),
    )
    state = start_state
    k_piece = lax.all_gather(key_rows, "sp", axis=0, tiled=True)
    v_piece = lax.all_gather(value, "sp", axis=0, tiled=True)
    block_count = k_piece.shape[0] // rows_here
    k_split = k_piece.reshape(block_count, rows_here, heads_here, head_dim)
    v_split = v_piece.reshape(block_count, rows_here, heads_here, head_dim)

    def visit(carry, item):
        k_blk, v_blk, block_idx = item
        k_first = block_idx * rows_here
        k_cum = lax.dynamic_slice_in_dim(cum_all, k_first, rows_here, 0).T

        def take_block(inner):
            return merge_terms(
                inner, block_terms(q_heads, cum_gate, k_blk, v_blk, k_cum, own_first, k_first)
            )

        def skip_block(inner):
            return inner

        return (lax.cond(k_first <= own_first, take_block, skip_block, carry), None)

    state, unused = lax.scan(
        visit, state, (k_split, v_split, jnp.arange(block_count, dtype=jnp.int32))
    )
    top_all, total_all, acc_all = state
    attn_out = (
        (acc_all / total_all[..., None])
        .transpose(1, 0, 2)
        .reshape(rows_here, attn_width)
        .astype(jnp.bfloat16)
    )
    log_total = top_all + jnp.log(total_all)
    mixed = lax.psum_scatter(
        (
            jnp.dot(conv_out, w_conv_out, preferred_element_type=jnp.float32)
            + jnp.dot(attn_out, w_attn_out, preferred_element_type=jnp.float32)
        ).astype(jnp.bfloat16),
        "tp",
        scatter_dimension=0,
        tiled=True,
    )
    return (mixed, log_total)


AG_CHUNKS = 4
OUT_CHUNKS = 4
MESH = pl.DeviceIdType.MESH
NT = (((1,), (1,)), ((), ()))


def fused_kernel(
    n_sp,
    n_tp,
    x_hbm,
    gain_ref,
    wci_hbm,
    wcg_hbm,
    ck_ref,
    lng_ref,
    wq_hbm,
    wk_hbm,
    wv_hbm,
    cum_ref,
    wco_hbm,
    wao_hbm,
    out_ref,
    log_ref,
    xg,
    xs,
    wbuf,
    wco,
    wao,
    acc,
    ss,
    zsend,
    zrecv,
    q_s,
    k_s,
    v_s,
    cum_recv,
    ext,
    glu_s,
    halo,
    csum,
    st_send,
    st_recv,
    cpart,
    ret_send,
    ret_recv,
    att_s,
    lse_send,
    lse_recv,
    d_send,
    d_recv,
    x_send,
    x_recv,
    parts,
    wsem,
    owsem,
    xsem,
    ag_send,
    ag_recv,
    zs_sem,
    zr_sem,
    cs_sem,
    cr_sem,
    hs_sem,
    hr_sem,
    ss_sem,
    sr_sem,
    rs_sem,
    rr_sem,
    ls_sem,
    lr_sem,
    ds_sem,
    dr_sem,
    xs_sem,
    xr_sem,
):
    f32, bf16 = jnp.float32, jnp.bfloat16
    z = lax.axis_index("sp")
    me = lax.axis_index("tp")
    chip, core = me // 2, me % 2
    chips = n_tp // 2
    rows, width = x_hbm.shape
    conv_w = wci_hbm.shape[0]
    attn_w = wq_hbm.shape[0]
    heads = n_sp
    hd = attn_w // heads
    d_all = wci_hbm.shape[1]
    partner = chip * 2 + 1 - core

    def remote(src, dst, s, r, dev):
        return pltpu.make_async_remote_copy(
            src_ref=src, dst_ref=dst, send_sem=s, recv_sem=r, device_id=dev, device_id_type=MESH
        )

    def same_core(dist):
        return lax.rem(chip + dist, chips) * 2 + core

    def other_core(dist):
        return lax.rem(chip + dist, chips) * 2 + 1 - core

    def piece_owner(rel):
        return same_core(rel // 2) if rel % 2 == 0 else other_core(rel // 2)

    def piece_source(rel):
        back = chips - rel // 2
        return same_core(back) if rel % 2 == 0 else other_core(back)

    barrier = pltpu.get_barrier_semaphore()
    for rel in range(1, n_tp):
        pl.semaphore_signal(
            barrier, inc=1, device_id={"tp": piece_owner(rel)}, device_id_type=MESH
        )
    for dist in range(1, n_sp):
        pl.semaphore_signal(
            barrier, inc=1, device_id={"sp": lax.rem(z + dist, n_sp)}, device_id_type=MESH
        )

    own_copy = pltpu.make_async_copy(x_hbm, xg.at[0], xsem)
    own_copy.start()
    loads = []
    for h in range(heads):
        loads.append((wq_hbm.at[pl.ds(h * hd, hd)], wbuf.at[pl.ds(2 * h * hd, hd)]))
        loads.append((wk_hbm.at[pl.ds(h * hd, hd)], wbuf.at[pl.ds((2 * h + 1) * hd, hd)]))
    loads.append((wv_hbm, wbuf.at[pl.ds(2 * attn_w, attn_w)]))
    qkv_loads = len(loads)
    qkv_w = 3 * attn_w
    loads.append((wci_hbm, wbuf.at[pl.ds(qkv_w, conv_w)]))
    loads.append((wcg_hbm, wbuf.at[pl.ds(qkv_w + conv_w, conv_w)]))
    wcopies = [pltpu.make_async_copy(a, b, wsem.at[i]) for i, (a, b) in enumerate(loads)]
    wco_copy = pltpu.make_async_copy(wco_hbm, wco, owsem.at[0])
    wao_copy = pltpu.make_async_copy(wao_hbm, wao, owsem.at[1])
    for c in wcopies:
        c.start()
    wco_copy.start()
    wao_copy.start()

    pl.semaphore_wait(barrier, n_tp - 1 + n_sp - 1)

    rc = rows // AG_CHUNKS

    def ag_copy(rel, kind, c):
        r = pl.ds(c * rc, rc)
        if kind == "own":
            return remote(
                x_hbm.at[r], xg.at[rel, r], ag_send.at[rel, c], ag_recv.at[rel, c],
                {"tp": piece_owner(rel)},
            )
        return remote(
            xg.at[rel - 1, r], xg.at[rel, r], ag_send.at[rel, c], ag_recv.at[rel, c],
            {"tp": partner},
        )

    ag = {}
    for c in range(AG_CHUNKS):
        for dist in range(1, chips):
            ag[2 * dist, c] = ag_copy(2 * dist, "own", c)
            ag[2 * dist, c].start()
    for c in range(AG_CHUNKS):
        ag[1, c] = ag_copy(1, "own", c)
        ag[1, c].start()
    cums = []
    for dist in range(1, n_sp):
        cp = remote(
            cum_ref, cum_recv.at[z], cs_sem.at[dist], cr_sem.at[dist],
            {"sp": lax.rem(z + dist, n_sp)},
        )
        cp.start()
        cums.append(cp)
    cum_recv[z] = cum_ref[...]

    def prepare(rel, c0, n):
        r = pl.ds(c0, n)
        owner = piece_source(rel)
        raw = xg[rel, r].astype(f32)
        g = gain_ref[pl.ds(pl.multiple_of(owner * width, width), width)].astype(f32).reshape(1, width)
        xs[rel, r] = (raw * g).astype(bf16)
        return jnp.sum(raw * raw, axis=1, keepdims=True)

    def wcols(rel, first, n):
        owner = piece_source(rel)
        return wbuf[pl.ds(first, n), pl.ds(pl.multiple_of(owner * width, width), width)]

    own_copy.wait()
    ss[...] = prepare(0, 0, rows)
    for c in wcopies[:qkv_loads]:
        c.wait()
    acc[:, :qkv_w] = lax.dot_general(xs[0], wcols(0, 0, qkv_w), NT, preferred_element_type=f32)
    for c in wcopies[qkv_loads:]:
        c.wait()
    acc[:, qkv_w:] = lax.dot_general(
        xs[0], wcols(0, qkv_w, 2 * conv_w), NT, preferred_element_type=f32
    )
    for c in range(AG_CHUNKS):
        ag[1, c].wait_recv()
    ss[...] += prepare(1, 0, rows)
    acc[...] += lax.dot_general(
        xs[1], wcols(1, 0, qkv_w + 2 * conv_w), NT, preferred_element_type=f32
    )

    half = rc // 2
    for c in range(AG_CHUNKS):
        r = pl.ds(c * rc, rc)
        for dist in range(1, chips):
            ag[2 * dist, c].wait_recv()
            ag[2 * dist + 1, c] = ag_copy(2 * dist + 1, "relay", c)
            ag[2 * dist + 1, c].start()
        total = acc[r, :qkv_w]
        sq = ss[r]
        for dist in range(1, chips):
            for rel in (2 * dist, 2 * dist + 1):
                if rel % 2 == 1:
                    ag[rel, c].wait_recv()
                sq = sq + prepare(rel, c * rc, rc)
                total = total + lax.dot_general(
                    xs[rel, r], wcols(rel, 0, qkv_w), NT, preferred_element_type=f32
                )
        rms = lax.rsqrt(sq / d_all + 1e-06)
        ss[r] = rms
        total = total * rms
        for h in range(heads):
            zsend[h, c, :rc] = total[:, 2 * h * hd : 2 * (h + 1) * hd].astype(bf16)
            v_h = total[:, 2 * attn_w + h * hd : 2 * attn_w + (h + 1) * hd]
            zsend[h, c, rc:] = jnp.concatenate([v_h[:half], v_h[half:]], axis=1).astype(bf16)
        for dist in range(n_sp - 1, 0, -1):
            to = lax.rem(z + dist, n_sp)
            remote(
                zsend.at[to, c], zrecv.at[z, c], zs_sem.at[dist, c], zr_sem.at[dist, c], {"sp": to}
            ).start()
        zrecv[z, c] = zsend[z, c]

    pre = acc[:, qkv_w:]
    for rel in range(2, n_tp):
        pre = pre + lax.dot_general(
            xs[rel], wcols(rel, qkv_w, 2 * conv_w), NT, preferred_element_type=f32
        )
    pre = pre * ss[...]
    glu = (pre[:, :conv_w] * jax.nn.sigmoid(pre[:, conv_w:])).astype(bf16)
    taps = ck_ref.shape[0]
    rim = halo.shape[0]
    glu_s[...] = glu
    halo_copy = remote(
        glu_s.at[pl.ds(rows - rim, rim)], halo, hs_sem, hr_sem, {"sp": lax.rem(z + 1, n_sp)}
    )

    @pl.when(z < n_sp - 1)
    def _():
        halo_copy.start()

    ext[rim:, :] = glu.astype(f32)
    blk = 64

    def conv_block(b, carry):
        first = pl.multiple_of(b * blk, blk)
        block = ext[pl.ds(first, blk + rim), :]
        tot = jnp.zeros((blk, conv_w), f32)
        for j in range(taps):
            off = rim - (taps - 1) + j
            tot = tot + block[off : off + blk] * ck_ref[j : j + 1, :].astype(f32)
        csum[pl.ds(first, blk), :] = tot
        return carry

    lax.fori_loop(1, rows // blk, conv_block, 0)
    for cp in cums:
        cp.wait_recv()
    for dist in range(n_sp - 1, 0, -1):
        for c in range(AG_CHUNKS):
            src = lax.rem(z + dist, n_sp)
            remote(
                zsend.at[src, c],
                zrecv.at[src, c],
                zs_sem.at[n_sp - dist, c],
                zr_sem.at[n_sp - dist, c],
                {"sp": src},
            ).wait_recv()
    for s in range(n_sp):
        for c in range(AG_CHUNKS):
            r0 = s * rows + c * rc
            tile = zrecv[s, c, :rc].astype(f32)
            q_s[pl.ds(r0, rc)] = tile[:, :hd].astype(bf16)
            k_s[pl.ds(r0, rc)] = tile[:, hd:].astype(bf16)
            vt = zrecv[s, c, rc:].astype(f32)
            v_s[pl.ds(r0, half)] = vt[:, :hd].astype(bf16)
            v_s[pl.ds(r0 + half, half)] = vt[:, hd:].astype(bf16)
    scale = hd ** (-0.5)
    hrows = rows // 2
    allowed = lax.broadcasted_iota(jnp.int32, (rows, rows), 1) <= lax.broadcasted_iota(
        jnp.int32, (rows, rows), 0
    )
    for i in range(n_sp - 1, -1, -1):
        keys = (i + 1) * rows
        q = q_s[pl.ds(i * rows, rows)]
        cum_k = jnp.concatenate([cum_recv[s, pl.ds(z, 1)] for s in range(i + 1)], axis=1)
        sc = lax.dot_general(q, k_s[:keys], NT, preferred_element_type=f32) * scale - cum_k
        diag = jnp.where(allowed, sc[:, keys - rows :], -jnp.inf)
        sc = diag if i == 0 else jnp.concatenate([sc[:, : keys - rows], diag], axis=1)
        top = jnp.max(sc, axis=1, keepdims=True)
        p = jnp.exp(sc - top)
        tot = jnp.sum(p, axis=1, keepdims=True)
        o = jnp.dot(p.astype(bf16), v_s[:keys], preferred_element_type=f32) / tot
        ret_send[i] = jnp.concatenate([o[:hrows], o[hrows:]], axis=1).astype(bf16)
        lse = jnp.broadcast_to(top + jnp.log(tot), (rows, 128)).T[:8]
        lse_send[i] = lse + cum_recv[i, pl.ds(z, 1)]

        @pl.when(z != i)
        def _():
            remote(
                ret_send.at[i], ret_recv.at[z], rs_sem.at[i], rr_sem.at[z], {"sp": i}
            ).start()
            remote(
                lse_send.at[i], lse_recv.at[z], ls_sem.at[i], lr_sem.at[z], {"sp": i}
            ).start()

        @pl.when(z == i)
        def _():
            ret_recv[i] = ret_send[i]
            lse_recv[i] = lse_send[i]


    @pl.when(z == 0)
    def _():
        halo[...] = jnp.zeros_like(halo)

    @pl.when(z > 0)
    def _():
        halo_copy.wait_recv()

    ext[:rim, :] = halo[...].astype(f32)
    conv_block(0, 0)
    cs = csum[...]
    first = jnp.sum(cs, axis=1, keepdims=True)
    second = jnp.sum(cs * cs, axis=1, keepdims=True)
    lane = lax.broadcasted_iota(jnp.int32, (rows, 128), 1)
    both = jnp.where(lane == 0, first, second)
    st_send[...] = both.T[: st_send.shape[0]]
    stats = []
    for rel in range(1, n_tp):
        cp = remote(
            st_send, st_recv.at[rel - 1], ss_sem.at[rel], sr_sem.at[rel], {"tp": piece_owner(rel)}
        )
        cp.start()
        stats.append(cp)
    tot = st_send[...]
    for rel in range(1, n_tp):
        stats[rel - 1].wait_recv()
        tot = tot + st_recv[rel - 1]
    wide = jnp.concatenate([tot] * (128 // tot.shape[0]), axis=0).T
    mean = wide[:, 0:1] / CONV_CH
    var = wide[:, 1:2] / CONV_CH - mean * mean
    normed = (csum[...] - mean) * lax.rsqrt(var + 1e-05) * lng_ref[...].astype(f32).reshape(1, conv_w)
    conv_out = (normed / (1.0 + jnp.exp(-normed))).astype(bf16)
    wco_copy.wait()
    cpart[...] = jnp.dot(conv_out, wco[...], preferred_element_type=f32)

    for h in range(n_sp):

        @pl.when(z != h)
        def _():
            remote(
                ret_send.at[h], ret_recv.at[h], rs_sem.at[h], rr_sem.at[h], {"sp": h}
            ).wait_recv()
            remote(
                lse_send.at[h], lse_recv.at[h], ls_sem.at[h], lr_sem.at[h], {"sp": h}
            ).wait_recv()

    got = [ret_recv[h].astype(f32) for h in range(n_sp)]
    att_s[:hrows] = jnp.concatenate([g[:, :hd] for g in got], axis=1).astype(bf16)
    att_s[hrows:] = jnp.concatenate([g[:, hd:] for g in got], axis=1).astype(bf16)
    for h in range(n_sp):
        log_ref[pl.ds(h, 1), :] = lse_recv[h, 0:1, :]
    wao_copy.wait()
    own_rows = rows // n_tp
    cw = d_all // OUT_CHUNKS
    mine = pl.ds(pl.multiple_of(core * own_rows, own_rows), own_rows)
    theirs = pl.ds(pl.multiple_of((1 - core) * own_rows, own_rows), own_rows)
    d2d, xc = {}, {}

    def exchange(dist):
        to_chip = lax.rem(chip + dist, chips)
        r = pl.ds(pl.multiple_of(to_chip * 2 * own_rows, 2 * own_rows), 2 * own_rows)
        for n in range(OUT_CHUNKS):
            cols = slice(n * cw, (n + 1) * cw)
            parts[dist, n] = cpart[r, cols] + jnp.dot(
                att_s[r, :], wao[:, cols], preferred_element_type=f32
            )
            d_send[dist, n] = parts[dist, n, theirs].astype(bf16)
            d2d[dist, n] = remote(
                d_send.at[dist, n],
                d_recv.at[dist, n],
                ds_sem.at[dist, n],
                dr_sem.at[dist, n],
                {"tp": partner},
            )
            d2d[dist, n].start()

    def forward(dist):
        for n in range(OUT_CHUNKS):
            d2d[dist, n].wait_recv()
            x_send[dist - 1, n] = (
                parts[dist, n, mine] + d_recv[dist, n].astype(f32)
            ).astype(bf16)
            xc[dist, n] = remote(
                x_send.at[dist - 1, n],
                x_recv.at[dist - 1, n],
                xs_sem.at[dist - 1, n],
                xr_sem.at[dist - 1, n],
                {"tp": same_core(dist)},
            )
            xc[dist, n].start()

    for dist in range(1, chips):
        exchange(dist)
    for dist in range(1, chips):
        forward(dist)
    exchange(0)
    for n in range(OUT_CHUNKS):
        d2d[0, n].wait_recv()
    for n in range(OUT_CHUNKS):
        tot = parts[0, n, mine] + d_recv[0, n].astype(f32)
        for dist in range(1, chips):
            xc[dist, n].wait_recv()
            tot = tot + x_recv[dist - 1, n].astype(f32)
        out_ref[:, n * cw : (n + 1) * cw] = tot.astype(bf16)

    for cp in list(ag.values()) + cums + stats + list(d2d.values()) + list(xc.values()):
        cp.wait_send()

    @pl.when(z < n_sp - 1)
    def _():
        halo_copy.wait_send()

    for dist in range(1, n_sp):
        to = lax.rem(z + dist, n_sp)
        for c in range(AG_CHUNKS):
            remote(
                zsend.at[to, c], zrecv.at[z, c], zs_sem.at[dist, c], zr_sem.at[dist, c], {"sp": to}
            ).wait_send()
    for i in range(n_sp):

        @pl.when(z != i)
        def _():
            remote(
                ret_send.at[i], ret_recv.at[z], rs_sem.at[i], rr_sem.at[z], {"sp": i}
            ).wait_send()
            remote(
                lse_send.at[i], lse_recv.at[z], ls_sem.at[i], lr_sem.at[z], {"sp": i}
            ).wait_send()


def fused_local(
    n_sp,
    n_tp,
    inputs,
    norm_gain,
    w_conv_in,
    w_conv_gate,
    conv_kernel,
    ln_gain,
    w_query,
    w_key,
    w_value,
    cum_gate,
    w_conv_out,
    w_attn_out,
):
    f32, bf16 = jnp.float32, jnp.bfloat16
    rows, width = inputs.shape
    conv_w, d_all = w_conv_in.shape
    attn_w = w_query.shape[0]
    heads = cum_gate.shape[0]
    hd = attn_w // heads
    chips = n_tp // 2
    own_rows = rows // n_tp
    rc = rows // AG_CHUNKS
    rim = -(-(conv_kernel.shape[0] - 1) // 16) * 16
    cw = d_all // OUT_CHUNKS
    all_w = 3 * attn_w + 2 * conv_w
    dma = pltpu.SemaphoreType.DMA
    scratch = [
        pltpu.VMEM((n_tp, rows, width), bf16),
        pltpu.VMEM((n_tp, rows, width), bf16),
        pltpu.VMEM((all_w, d_all), bf16),
        pltpu.VMEM((conv_w, d_all), bf16),
        pltpu.VMEM((attn_w, d_all), bf16),
        pltpu.VMEM((rows, all_w), f32),
        pltpu.VMEM((rows, 1), f32),
        pltpu.VMEM((n_sp, AG_CHUNKS, rc + rc // 2, 2 * hd), bf16),
        pltpu.VMEM((n_sp, AG_CHUNKS, rc + rc // 2, 2 * hd), bf16),
        pltpu.VMEM((n_sp * rows, hd), bf16),
        pltpu.VMEM((n_sp * rows, hd), bf16),
        pltpu.VMEM((n_sp * rows, hd), bf16),
        pltpu.VMEM((n_sp, heads, rows), f32),
        pltpu.VMEM((rows + rim, conv_w), f32),
        pltpu.VMEM((rows, conv_w), bf16),
        pltpu.VMEM((rim, conv_w), bf16),
        pltpu.VMEM((rows, conv_w), f32),
        pltpu.VMEM((8, rows), f32),
        pltpu.VMEM((n_tp - 1, 8, rows), f32),
        pltpu.VMEM((rows, d_all), f32),
        pltpu.VMEM((n_sp, rows // 2, 2 * hd), bf16),
        pltpu.VMEM((n_sp, rows // 2, 2 * hd), bf16),
        pltpu.VMEM((rows, attn_w), bf16),
        pltpu.VMEM((n_sp, 8, rows), f32),
        pltpu.VMEM((n_sp, 8, rows), f32),
        pltpu.VMEM((chips, OUT_CHUNKS, own_rows, cw), bf16),
        pltpu.VMEM((chips, OUT_CHUNKS, own_rows, cw), bf16),
        pltpu.VMEM((chips - 1, OUT_CHUNKS, own_rows, cw), bf16),
        pltpu.VMEM((chips - 1, OUT_CHUNKS, own_rows, cw), bf16),
        pltpu.VMEM((chips, OUT_CHUNKS, 2 * own_rows, cw), f32),
        dma((2 * heads + 3,)),
        dma((2,)),
        dma,
        dma((n_tp, AG_CHUNKS)),
        dma((n_tp, AG_CHUNKS)),
        dma((n_sp, AG_CHUNKS)),
        dma((n_sp, AG_CHUNKS)),
        dma((n_sp,)),
        dma((n_sp,)),
        dma,
        dma,
        dma((n_tp,)),
        dma((n_tp,)),
        dma((n_sp,)),
        dma((n_sp,)),
        dma((n_sp,)),
        dma((n_sp,)),
        dma((chips, OUT_CHUNKS)),
        dma((chips, OUT_CHUNKS)),
        dma((chips - 1, OUT_CHUNKS)),
        dma((chips - 1, OUT_CHUNKS)),
    ]
    far = pl.BlockSpec(memory_space=pl.ANY)
    near = pl.BlockSpec(memory_space=pltpu.VMEM)
    mixed, log_total = pl.pallas_call(
        functools.partial(fused_kernel, n_sp, n_tp),
        out_shape=(
            pltpu.VMEM((own_rows, d_all), bf16),
            pltpu.VMEM((heads, rows), f32),
        ),
        in_specs=[far, near, far, far, near, near, far, far, far, near, far, far],
        out_specs=(near, near),
        scratch_shapes=scratch,
        compiler_params=pltpu.CompilerParams(
            collective_id=0, has_side_effects=True, vmem_limit_bytes=60 * 1024 * 1024
        ),
    )(
        inputs,
        norm_gain,
        w_conv_in,
        w_conv_gate,
        conv_kernel,
        ln_gain,
        w_query,
        w_key,
        w_value,
        cum_gate,
        w_conv_out,
        w_attn_out,
    )
    return (mixed, log_total)


def solution(mesh):
    in_specs = (
        P(("grp", "sp"), "tp"),
        P(),
        P("tp", None),
        P("tp", None),
        P(None, "tp"),
        P("tp"),
        P("tp", None),
        P("tp", None),
        P("tp", None),
        P("tp", ("grp", "sp")),
        P("tp", None),
        P("tp", None),
    )
    out_specs = (P(("grp", "sp", "tp"), None), P("tp", ("grp", "sp")))
    heads_here = HEADS // mesh.shape["tp"]
    fits = heads_here == mesh.shape["sp"] and mesh.shape["tp"] % 2 == 0
    body = functools.partial(fused_local, mesh.shape["sp"], mesh.shape["tp"]) if fits else local
    return jax.shard_map(body, mesh=mesh, in_specs=in_specs, out_specs=out_specs, check_vma=False)
```

```python
import functools
import jax
import jax.numpy as jnp
from jax import lax
from jax.experimental import pallas as pl
from jax.experimental.pallas import tpu as pltpu
from jax.sharding import PartitionSpec as P

D = 2048
CONV_CH = 1024
HEADS = 16


neg_large = -1e30


def passed_along(block, axis, distance):
    devices = range(lax.axis_size(axis))
    route = [(i - distance, i) for i in devices if i - distance in devices]
    return lax.ppermute(block, axis, route)


def block_terms(q_blk, q_cum, k_blk, v_blk, k_cum, q_first, k_first):
    score_scale = q_blk.shape[2] ** (-0.5)
    scores = (
        jnp.einsum("qhd,khd->hqk", q_blk, k_blk, preferred_element_type=jnp.float32) * score_scale
    )
    scores = scores + q_cum[:, :, None] - k_cum[:, None, :]
    q_pos = q_first + jnp.arange(q_blk.shape[0], dtype=jnp.int32)
    k_pos = k_first + jnp.arange(k_blk.shape[0], dtype=jnp.int32)
    allowed = k_pos[None, :] <= q_pos[:, None]
    scores = jnp.where(allowed[None], scores, -jnp.inf)
    block_top = jnp.max(scores, axis=-1)
    weights = jnp.exp(scores - block_top[..., None])
    block_total = jnp.sum(weights, axis=-1)
    block_out = jnp.einsum(
        "hqk,khd->hqd", weights.astype(jnp.bfloat16), v_blk, preferred_element_type=jnp.float32
    ).astype(jnp.bfloat16)
    return (block_top, block_total, block_out)


def merge_terms(state, terms):
    top_now, total_now, acc_now = state
    block_top, block_total, block_out = terms
    top_new = jnp.maximum(top_now, block_top)
    keep_old = jnp.exp(top_now - top_new)
    keep_new = jnp.exp(block_top - top_new)
    return (
        top_new,
        total_now * keep_old + block_total * keep_new,
        acc_now * keep_old[..., None] + block_out.astype(jnp.float32) * keep_new[..., None],
    )


def local(
    inputs,
    norm_gain,
    w_conv_in,
    w_conv_gate,
    conv_kernel,
    ln_gain,
    w_query,
    w_key,
    w_value,
    cum_gate,
    w_conv_out,
    w_attn_out,
):
    rows_here = inputs.shape[0]
    conv_width = w_conv_in.shape[0]
    attn_width = w_query.shape[0]
    heads_here = cum_gate.shape[0]
    head_dim = attn_width // heads_here
    taps_count = conv_kernel.shape[0]
    w_all = jnp.concatenate([w_conv_in, w_conv_gate, w_query, w_key, w_value], axis=0)
    gain_all = norm_gain.astype(jnp.float32)
    contract_dims = (((1,), (1,)), ((), ()))
    piece_f = lax.all_gather(inputs, "tp", axis=1, tiled=True).astype(jnp.float32)
    scaled_piece = (piece_f * gain_all[None, :]).astype(jnp.bfloat16)
    raw_proj = lax.dot_general(
        scaled_piece, w_all, contract_dims, preferred_element_type=jnp.float32
    )
    squares = jnp.sum(piece_f * piece_f, axis=1)
    rms = lax.rsqrt(squares / D + 1e-06)[:, None]
    proj = raw_proj * rms
    conv_in = proj[:, :conv_width]
    conv_gate = proj[:, conv_width : 2 * conv_width]
    query = proj[:, 2 * conv_width : 2 * conv_width + attn_width].astype(jnp.bfloat16)
    key_rows = proj[:, 2 * conv_width + attn_width : 2 * conv_width + 2 * attn_width].astype(
        jnp.bfloat16
    )
    value = proj[:, 2 * conv_width + 2 * attn_width :].astype(jnp.bfloat16)
    glu = (conv_in * jax.nn.sigmoid(conv_gate)).astype(jnp.bfloat16)
    rim_rows = passed_along(glu[rows_here - (taps_count - 1) :], "sp", 1)
    extended = jnp.concatenate([rim_rows, glu], axis=0)
    kernel = conv_kernel.astype(jnp.float32)
    conv_sum = jnp.zeros((rows_here, conv_width), jnp.float32)
    for tap_idx in range(taps_count):
        conv_sum = (
            conv_sum
            + extended[tap_idx : tap_idx + rows_here].astype(jnp.float32) * kernel[tap_idx][None, :]
        )
    chan_first, chan_second = lax.psum(
        (jnp.sum(conv_sum, axis=1), jnp.sum(conv_sum * conv_sum, axis=1)), "tp"
    )
    chan_mean = (chan_first / CONV_CH)[:, None]
    chan_var = (chan_second / CONV_CH)[:, None] - chan_mean * chan_mean
    normed = (
        (conv_sum - chan_mean) * lax.rsqrt(chan_var + 1e-05) * ln_gain.astype(jnp.float32)[None, :]
    )
    conv_out = jax.nn.silu(normed).astype(jnp.bfloat16)
    q_heads = query.reshape(rows_here, heads_here, head_dim)
    cum_all = lax.all_gather(cum_gate.T, "sp", axis=0, tiled=True)
    own_first = lax.axis_index("sp") * rows_here
    start_state = (
        jnp.full((heads_here, rows_here), neg_large, jnp.float32),
        jnp.zeros((heads_here, rows_here), jnp.float32),
        jnp.zeros((heads_here, rows_here, head_dim), jnp.float32),
    )
    state = start_state
    k_piece = lax.all_gather(key_rows, "sp", axis=0, tiled=True)
    v_piece = lax.all_gather(value, "sp", axis=0, tiled=True)
    block_count = k_piece.shape[0] // rows_here
    k_split = k_piece.reshape(block_count, rows_here, heads_here, head_dim)
    v_split = v_piece.reshape(block_count, rows_here, heads_here, head_dim)

    def visit(carry, item):
        k_blk, v_blk, block_idx = item
        k_first = block_idx * rows_here
        k_cum = lax.dynamic_slice_in_dim(cum_all, k_first, rows_here, 0).T

        def take_block(inner):
            return merge_terms(
                inner, block_terms(q_heads, cum_gate, k_blk, v_blk, k_cum, own_first, k_first)
            )

        def skip_block(inner):
            return inner

        return (lax.cond(k_first <= own_first, take_block, skip_block, carry), None)

    state, unused = lax.scan(
        visit, state, (k_split, v_split, jnp.arange(block_count, dtype=jnp.int32))
    )
    top_all, total_all, acc_all = state
    attn_out = (
        (acc_all / total_all[..., None])
        .transpose(1, 0, 2)
        .reshape(rows_here, attn_width)
        .astype(jnp.bfloat16)
    )
    log_total = top_all + jnp.log(total_all)
    mixed = lax.psum_scatter(
        (
            jnp.dot(conv_out, w_conv_out, preferred_element_type=jnp.float32)
            + jnp.dot(attn_out, w_attn_out, preferred_element_type=jnp.float32)
        ).astype(jnp.bfloat16),
        "tp",
        scatter_dimension=0,
        tiled=True,
    )
    return (mixed, log_total)


AG_CHUNKS = 8
OUT_CHUNKS = 4
MESH = pl.DeviceIdType.MESH
NT = (((1,), (1,)), ((), ()))


def fused_kernel(
    n_sp,
    n_tp,
    x_hbm,
    gain_ref,
    wci_hbm,
    wcg_hbm,
    ck_ref,
    lng_ref,
    wq_hbm,
    wk_hbm,
    wv_hbm,
    cum_ref,
    wco_hbm,
    wao_hbm,
    out_ref,
    log_ref,
    xg,
    xs,
    wbuf,
    wco,
    wao,
    acc,
    ss,
    zsend,
    zrecv,
    q_s,
    k_s,
    v_s,
    v_t,
    cum_col,
    cum_recv,
    ext,
    halo_src,
    halo,
    csum,
    st_send,
    st_recv,
    cpart,
    ret_send,
    ret_recv,
    att_s,
    lse_send,
    lse_recv,
    d_send,
    d_recv,
    x_send,
    x_recv,
    parts,
    wsem,
    owsem,
    xsem,
    ag_send,
    ag_recv,
    zs_sem,
    zr_sem,
    cs_sem,
    cr_sem,
    hs_sem,
    hr_sem,
    ss_sem,
    sr_sem,
    rs_sem,
    rr_sem,
    ls_sem,
    lr_sem,
    ds_sem,
    dr_sem,
    xs_sem,
    xr_sem,
):
    f32, bf16 = jnp.float32, jnp.bfloat16
    z = lax.axis_index("sp")
    me = lax.axis_index("tp")
    chip, core = me // 2, me % 2
    chips = n_tp // 2
    rows, width = x_hbm.shape
    conv_w = wci_hbm.shape[0]
    attn_w = wq_hbm.shape[0]
    heads = n_sp
    hd = attn_w // heads
    d_all = wci_hbm.shape[1]
    partner = chip * 2 + 1 - core

    def remote(src, dst, s, r, dev):
        return pltpu.make_async_remote_copy(
            src_ref=src, dst_ref=dst, send_sem=s, recv_sem=r, device_id=dev, device_id_type=MESH
        )

    def same_core(dist):
        return lax.rem(chip + dist, chips) * 2 + core

    def other_core(dist):
        return lax.rem(chip + dist, chips) * 2 + 1 - core

    def piece_owner(rel):
        return same_core(rel // 2) if rel % 2 == 0 else other_core(rel // 2)

    def piece_source(rel):
        back = chips - rel // 2
        return same_core(back) if rel % 2 == 0 else other_core(back)

    barrier = pltpu.get_barrier_semaphore()
    for rel in range(1, n_tp):
        pl.semaphore_signal(
            barrier, inc=1, device_id={"tp": piece_owner(rel)}, device_id_type=MESH
        )
    for dist in range(1, n_sp):
        pl.semaphore_signal(
            barrier, inc=1, device_id={"sp": lax.rem(z + dist, n_sp)}, device_id_type=MESH
        )

    own_copy = pltpu.make_async_copy(x_hbm, xg.at[0], xsem)
    own_copy.start()
    loads = []
    for h in range(heads):
        loads.append((wq_hbm.at[pl.ds(h * hd, hd)], wbuf.at[pl.ds(2 * h * hd, hd)]))
        loads.append((wk_hbm.at[pl.ds(h * hd, hd)], wbuf.at[pl.ds((2 * h + 1) * hd, hd)]))
    loads.append((wv_hbm, wbuf.at[pl.ds(2 * attn_w, attn_w)]))
    qkv_loads = len(loads)
    qkv_w = 3 * attn_w
    loads.append((wci_hbm, wbuf.at[pl.ds(qkv_w, conv_w)]))
    loads.append((wcg_hbm, wbuf.at[pl.ds(qkv_w + conv_w, conv_w)]))
    wcopies = [pltpu.make_async_copy(a, b, wsem.at[i]) for i, (a, b) in enumerate(loads)]
    wco_copy = pltpu.make_async_copy(wco_hbm, wco, owsem.at[0])
    wao_copy = pltpu.make_async_copy(wao_hbm, wao, owsem.at[1])
    for c in wcopies:
        c.start()
    wco_copy.start()
    wao_copy.start()

    pl.semaphore_wait(barrier, n_tp - 1 + n_sp - 1)

    rc = rows // AG_CHUNKS

    def ag_copy(rel, kind, c):
        r = pl.ds(c * rc, rc)
        if kind == "own":
            return remote(
                x_hbm.at[r], xg.at[rel, r], ag_send.at[rel, c], ag_recv.at[rel, c],
                {"tp": piece_owner(rel)},
            )
        return remote(
            xg.at[rel - 1, r], xg.at[rel, r], ag_send.at[rel, c], ag_recv.at[rel, c],
            {"tp": partner},
        )

    order = [AG_CHUNKS - 1] + list(range(AG_CHUNKS - 1))
    ag = {}
    for c in order:
        for dist in range(1, chips):
            ag[2 * dist, c] = ag_copy(2 * dist, "own", c)
            ag[2 * dist, c].start()
    for c in order:
        ag[1, c] = ag_copy(1, "own", c)
        ag[1, c].start()
    cums = []
    for dist in range(1, n_sp):
        cp = remote(
            cum_ref, cum_recv.at[z], cs_sem.at[dist], cr_sem.at[dist],
            {"sp": lax.rem(z + dist, n_sp)},
        )
        cp.start()
        cums.append(cp)
    cum_recv[z] = cum_ref[...]

    def prepare(rel, c0, n):
        r = pl.ds(c0, n)
        owner = piece_source(rel)
        raw = xg[rel, r].astype(f32)
        g = gain_ref[pl.ds(pl.multiple_of(owner * width, width), width)].astype(f32).reshape(1, width)
        xs[rel, r] = (raw * g).astype(bf16)
        return jnp.sum(raw * raw, axis=1, keepdims=True)

    def wcols(rel, first, n):
        owner = piece_source(rel)
        return wbuf[pl.ds(first, n), pl.ds(pl.multiple_of(owner * width, width), width)]

    own_copy.wait()
    ss[...] = prepare(0, 0, rows)
    for c in wcopies[:qkv_loads]:
        c.wait()
    acc[:, :qkv_w] = lax.dot_general(xs[0], wcols(0, 0, qkv_w), NT, preferred_element_type=f32)
    for c in wcopies[qkv_loads:]:
        c.wait()
    acc[:, qkv_w:] = lax.dot_general(
        xs[0], wcols(0, qkv_w, 2 * conv_w), NT, preferred_element_type=f32
    )
    for c in range(AG_CHUNKS):
        ag[1, c].wait_recv()
    ss[...] += prepare(1, 0, rows)
    acc[...] += lax.dot_general(
        xs[1], wcols(1, 0, qkv_w + 2 * conv_w), NT, preferred_element_type=f32
    )

    half = rc // 2

    def finish_chunk(c):
        r = pl.ds(c * rc, rc)
        total = acc[r, :qkv_w]
        sq = ss[r]
        for dist in range(1, chips):
            ag[2 * dist + 1, c].wait_recv()
            sq = sq + prepare(2 * dist + 1, c * rc, rc)
            total = total + lax.dot_general(
                xs[2 * dist + 1, r],
                wcols(2 * dist + 1, 0, qkv_w),
                NT,
                preferred_element_type=f32,
            )
        rms = lax.rsqrt(sq / d_all + 1e-06)
        ss[r] = rms
        total = total * rms
        for h in range(heads):
            zsend[h, c, :rc] = total[:, 2 * h * hd : 2 * (h + 1) * hd].astype(bf16)
            v_h = total[:, 2 * attn_w + h * hd : 2 * attn_w + (h + 1) * hd]
            zsend[h, c, rc:] = jnp.concatenate([v_h[:half], v_h[half:]], axis=1).astype(bf16)
        for dist in range(n_sp - 1, 0, -1):
            to = lax.rem(z + dist, n_sp)
            remote(
                zsend.at[to, c], zrecv.at[z, c], zs_sem.at[dist, c], zr_sem.at[dist, c], {"sp": to}
            ).start()
        zrecv[z, c] = zsend[z, c]

    rim = halo.shape[0]
    halo_copy = remote(
        halo_src, halo, hs_sem, hr_sem, {"sp": lax.rem(z + 1, n_sp)}
    )

    def gated(r):
        pre = acc[r, qkv_w:]
        for rel in range(2, n_tp):
            pre = pre + lax.dot_general(
                xs[rel, r], wcols(rel, qkv_w, 2 * conv_w), NT, preferred_element_type=f32
            )
        pre = pre * ss[r]
        return (pre[:, :conv_w] * jax.nn.sigmoid(pre[:, conv_w:])).astype(bf16)

    for k, c in enumerate(order):
        r = pl.ds(c * rc, rc)
        for dist in range(1, chips):
            ag[2 * dist, c].wait_recv()
            ag[2 * dist + 1, c] = ag_copy(2 * dist + 1, "relay", c)
            ag[2 * dist + 1, c].start()
        for dist in range(1, chips):
            ss[r] += prepare(2 * dist, c * rc, rc)
            acc[r, :qkv_w] += lax.dot_general(
                xs[2 * dist, r], wcols(2 * dist, 0, qkv_w), NT, preferred_element_type=f32
            )
        if k == 0:
            finish_chunk(c)
        elif k == 1:
            halo_src[...] = gated(pl.ds(rows - rim, rim))

            @pl.when(z < n_sp - 1)
            def _():
                halo_copy.start()

        else:
            finish_chunk(order[k - 1])
    finish_chunk(order[-1])

    glu = gated(pl.ds(0, rows))
    taps = ck_ref.shape[0]
    ext[rim:, :] = glu.astype(f32)
    blk = 64

    def conv_block(b, carry):
        first = pl.multiple_of(b * blk, blk)
        block = ext[pl.ds(first, blk + rim), :]
        tot = jnp.zeros((blk, conv_w), f32)
        for j in range(taps):
            off = rim - (taps - 1) + j
            tot = tot + block[off : off + blk] * ck_ref[j : j + 1, :].astype(f32)
        csum[pl.ds(first, blk), :] = tot
        return carry

    lax.fori_loop(1, rows // blk, conv_block, 0)
    for cp in cums:
        cp.wait_recv()
    for src in range(n_sp):
        cum_col[pl.ds(src * rows, rows)] = jnp.broadcast_to(
            cum_recv[src, pl.ds(z, 1)], (128, rows)
        ).T

    @pl.when(z == 0)
    def _():
        halo[...] = jnp.zeros_like(halo)

    @pl.when(z > 0)
    def _():
        halo_copy.wait_recv()

    ext[:rim, :] = halo[...].astype(f32)
    conv_block(0, 0)
    cs = csum[...]
    first = jnp.sum(cs, axis=1, keepdims=True)
    second = jnp.sum(cs * cs, axis=1, keepdims=True)
    lane = lax.broadcasted_iota(jnp.int32, (rows, 128), 1)
    both = jnp.where(lane == 0, first, second)
    st_send[...] = both.T[: st_send.shape[0]]
    stats = []
    for rel in range(1, n_tp):
        cp = remote(
            st_send, st_recv.at[rel - 1], ss_sem.at[rel], sr_sem.at[rel], {"tp": piece_owner(rel)}
        )
        cp.start()
        stats.append(cp)
    for dist in range(n_sp - 1, 0, -1):
        for c in range(AG_CHUNKS):
            src = lax.rem(z + dist, n_sp)
            remote(
                zsend.at[src, c],
                zrecv.at[src, c],
                zs_sem.at[n_sp - dist, c],
                zr_sem.at[n_sp - dist, c],
                {"sp": src},
            ).wait_recv()
    scale = hd ** (-0.5)
    low = lax.broadcasted_iota(jnp.int32, (half, 2 * hd), 1) < hd
    for s in range(n_sp):
        for c in range(AG_CHUNKS):
            r0 = s * rows + c * rc
            tile = zrecv[s, c, :rc].astype(f32)
            q_s[pl.ds(r0, rc)] = (tile[:, :hd] * scale).astype(bf16)
            k_s[pl.ds(r0, rc)] = tile[:, hd:].astype(bf16)
            vt = zrecv[s, c, rc:].astype(f32)
            v_s[pl.ds(r0, half)] = jnp.where(low, vt, 1.0).astype(bf16)
            v_s[pl.ds(r0 + half, half)] = jnp.where(low, pltpu.roll(vt, hd, 1), 1.0).astype(bf16)
    v_t[...] = v_s[...].T
    wide_k = -(-rows // 128)
    allowed = lax.broadcasted_iota(jnp.int32, (rows, rows), 0) <= lax.broadcasted_iota(
        jnp.int32, (rows, rows), 1
    )
    for i in [k // 2 if k % 2 == 0 else n_sp - 1 - k // 2 for k in range(n_sp)]:
        keys = (i + 1) * rows
        q = q_s[pl.ds(i * rows, rows)]
        cum_k = jnp.concatenate([cum_col[:keys]] * wide_k, axis=1)
        sc = lax.dot_general(k_s[:keys], q, NT, preferred_element_type=f32) - cum_k
        diag = jnp.where(allowed, sc[keys - rows :], -jnp.inf)
        sc = diag if i == 0 else jnp.concatenate([sc[: keys - rows], diag], axis=0)
        top = jnp.max(sc, axis=0, keepdims=True)
        p = jnp.exp(sc - top).astype(bf16)
        both = jnp.dot(v_t[:, :keys], p, preferred_element_type=f32)
        tot = both[hd : hd + 1]
        ret_send[i] = (both[:hd] / tot).astype(bf16)
        lse = top + jnp.log(tot) + cum_recv[i, pl.ds(z, 1)]
        lse_send[i] = jnp.broadcast_to(lse, (8, rows))

        @pl.when(z != i)
        def _():
            remote(
                ret_send.at[i], ret_recv.at[z], rs_sem.at[i], rr_sem.at[z], {"sp": i}
            ).start()
            remote(
                lse_send.at[i], lse_recv.at[z], ls_sem.at[i], lr_sem.at[z], {"sp": i}
            ).start()

        @pl.when(z == i)
        def _():
            ret_recv[i] = ret_send[i]
            lse_recv[i] = lse_send[i]

    tot = st_send[...]
    for rel in range(1, n_tp):
        stats[rel - 1].wait_recv()
        tot = tot + st_recv[rel - 1]
    wide = jnp.concatenate([tot] * (128 // tot.shape[0]), axis=0).T
    mean = wide[:, 0:1] / CONV_CH
    var = wide[:, 1:2] / CONV_CH - mean * mean
    normed = (csum[...] - mean) * lax.rsqrt(var + 1e-05) * lng_ref[...].astype(f32).reshape(1, conv_w)
    conv_out = (normed / (1.0 + jnp.exp(-normed))).astype(bf16)
    wco_copy.wait()
    cpart[...] = jnp.dot(conv_out, wco[...], preferred_element_type=f32)

    for h in range(n_sp):

        @pl.when(z != h)
        def _():
            remote(
                ret_send.at[h], ret_recv.at[h], rs_sem.at[h], rr_sem.at[h], {"sp": h}
            ).wait_recv()
            remote(
                lse_send.at[h], lse_recv.at[h], ls_sem.at[h], lr_sem.at[h], {"sp": h}
            ).wait_recv()

    att_s[...] = jnp.concatenate([ret_recv[h] for h in range(n_sp)], axis=0).astype(f32).T.astype(bf16)
    for h in range(n_sp):
        log_ref[pl.ds(h, 1), :] = lse_recv[h, 0:1, :]
    wao_copy.wait()
    own_rows = rows // n_tp
    cw = d_all // OUT_CHUNKS
    mine = pl.ds(pl.multiple_of(core * own_rows, own_rows), own_rows)
    theirs = pl.ds(pl.multiple_of((1 - core) * own_rows, own_rows), own_rows)
    d2d, xc = {}, {}

    def exchange(dist):
        to_chip = lax.rem(chip + dist, chips)
        r = pl.ds(pl.multiple_of(to_chip * 2 * own_rows, 2 * own_rows), 2 * own_rows)
        for n in range(OUT_CHUNKS):
            cols = slice(n * cw, (n + 1) * cw)
            parts[dist, n] = cpart[r, cols] + jnp.dot(
                att_s[r, :], wao[:, cols], preferred_element_type=f32
            )
            d_send[dist, n] = parts[dist, n, theirs].astype(bf16)
            d2d[dist, n] = remote(
                d_send.at[dist, n],
                d_recv.at[dist, n],
                ds_sem.at[dist, n],
                dr_sem.at[dist, n],
                {"tp": partner},
            )
            d2d[dist, n].start()

    def forward(dist):
        for n in range(OUT_CHUNKS):
            d2d[dist, n].wait_recv()
            x_send[dist - 1, n] = (
                parts[dist, n, mine] + d_recv[dist, n].astype(f32)
            ).astype(bf16)
            xc[dist, n] = remote(
                x_send.at[dist - 1, n],
                x_recv.at[dist - 1, n],
                xs_sem.at[dist - 1, n],
                xr_sem.at[dist - 1, n],
                {"tp": same_core(dist)},
            )
            xc[dist, n].start()

    for dist in range(1, chips):
        exchange(dist)
    for dist in range(1, chips):
        forward(dist)
    exchange(0)
    for n in range(OUT_CHUNKS):
        d2d[0, n].wait_recv()
    for n in range(OUT_CHUNKS):
        tot = parts[0, n, mine] + d_recv[0, n].astype(f32)
        for dist in range(1, chips):
            xc[dist, n].wait_recv()
            tot = tot + x_recv[dist - 1, n].astype(f32)
        out_ref[:, n * cw : (n + 1) * cw] = tot.astype(bf16)

    for cp in list(ag.values()) + cums + stats + list(d2d.values()) + list(xc.values()):
        cp.wait_send()

    @pl.when(z < n_sp - 1)
    def _():
        halo_copy.wait_send()

    for dist in range(1, n_sp):
        to = lax.rem(z + dist, n_sp)
        for c in range(AG_CHUNKS):
            remote(
                zsend.at[to, c], zrecv.at[z, c], zs_sem.at[dist, c], zr_sem.at[dist, c], {"sp": to}
            ).wait_send()
    for i in range(n_sp):

        @pl.when(z != i)
        def _():
            remote(
                ret_send.at[i], ret_recv.at[z], rs_sem.at[i], rr_sem.at[z], {"sp": i}
            ).wait_send()
            remote(
                lse_send.at[i], lse_recv.at[z], ls_sem.at[i], lr_sem.at[z], {"sp": i}
            ).wait_send()


def fused_local(
    n_sp,
    n_tp,
    inputs,
    norm_gain,
    w_conv_in,
    w_conv_gate,
    conv_kernel,
    ln_gain,
    w_query,
    w_key,
    w_value,
    cum_gate,
    w_conv_out,
    w_attn_out,
):
    f32, bf16 = jnp.float32, jnp.bfloat16
    rows, width = inputs.shape
    conv_w, d_all = w_conv_in.shape
    attn_w = w_query.shape[0]
    heads = cum_gate.shape[0]
    hd = attn_w // heads
    chips = n_tp // 2
    own_rows = rows // n_tp
    rc = rows // AG_CHUNKS
    rim = -(-(conv_kernel.shape[0] - 1) // 16) * 16
    cw = d_all // OUT_CHUNKS
    all_w = 3 * attn_w + 2 * conv_w
    dma = pltpu.SemaphoreType.DMA
    scratch = [
        pltpu.VMEM((n_tp, rows, width), bf16),
        pltpu.VMEM((n_tp, rows, width), bf16),
        pltpu.VMEM((all_w, d_all), bf16),
        pltpu.VMEM((conv_w, d_all), bf16),
        pltpu.VMEM((attn_w, d_all), bf16),
        pltpu.VMEM((rows, all_w), f32),
        pltpu.VMEM((rows, 1), f32),
        pltpu.VMEM((n_sp, AG_CHUNKS, rc + rc // 2, 2 * hd), bf16),
        pltpu.VMEM((n_sp, AG_CHUNKS, rc + rc // 2, 2 * hd), bf16),
        pltpu.VMEM((n_sp * rows, hd), bf16),
        pltpu.VMEM((n_sp * rows, hd), bf16),
        pltpu.VMEM((n_sp * rows, 2 * hd), bf16),
        pltpu.VMEM((2 * hd, n_sp * rows), bf16),
        pltpu.VMEM((n_sp * rows, 128), f32),
        pltpu.VMEM((n_sp, heads, rows), f32),
        pltpu.VMEM((rows + rim, conv_w), f32),
        pltpu.VMEM((rim, conv_w), bf16),
        pltpu.VMEM((rim, conv_w), bf16),
        pltpu.VMEM((rows, conv_w), f32),
        pltpu.VMEM((8, rows), f32),
        pltpu.VMEM((n_tp - 1, 8, rows), f32),
        pltpu.VMEM((rows, d_all), f32),
        pltpu.VMEM((n_sp, hd, rows), bf16),
        pltpu.VMEM((n_sp, hd, rows), bf16),
        pltpu.VMEM((rows, attn_w), bf16),
        pltpu.VMEM((n_sp, 8, rows), f32),
        pltpu.VMEM((n_sp, 8, rows), f32),
        pltpu.VMEM((chips, OUT_CHUNKS, own_rows, cw), bf16),
        pltpu.VMEM((chips, OUT_CHUNKS, own_rows, cw), bf16),
        pltpu.VMEM((chips - 1, OUT_CHUNKS, own_rows, cw), bf16),
        pltpu.VMEM((chips - 1, OUT_CHUNKS, own_rows, cw), bf16),
        pltpu.VMEM((chips, OUT_CHUNKS, 2 * own_rows, cw), f32),
        dma((2 * heads + 3,)),
        dma((2,)),
        dma,
        dma((n_tp, AG_CHUNKS)),
        dma((n_tp, AG_CHUNKS)),
        dma((n_sp, AG_CHUNKS)),
        dma((n_sp, AG_CHUNKS)),
        dma((n_sp,)),
        dma((n_sp,)),
        dma,
        dma,
        dma((n_tp,)),
        dma((n_tp,)),
        dma((n_sp,)),
        dma((n_sp,)),
        dma((n_sp,)),
        dma((n_sp,)),
        dma((chips, OUT_CHUNKS)),
        dma((chips, OUT_CHUNKS)),
        dma((chips - 1, OUT_CHUNKS)),
        dma((chips - 1, OUT_CHUNKS)),
    ]
    far = pl.BlockSpec(memory_space=pl.ANY)
    near = pl.BlockSpec(memory_space=pltpu.VMEM)
    mixed, log_total = pl.pallas_call(
        functools.partial(fused_kernel, n_sp, n_tp),
        out_shape=(
            pltpu.VMEM((own_rows, d_all), bf16),
            pltpu.VMEM((heads, rows), f32),
        ),
        in_specs=[far, near, far, far, near, near, far, far, far, near, far, far],
        out_specs=(near, near),
        scratch_shapes=scratch,
        compiler_params=pltpu.CompilerParams(
            collective_id=0, has_side_effects=True, vmem_limit_bytes=60 * 1024 * 1024
        ),
    )(
        inputs,
        norm_gain,
        w_conv_in,
        w_conv_gate,
        conv_kernel,
        ln_gain,
        w_query,
        w_key,
        w_value,
        cum_gate,
        w_conv_out,
        w_attn_out,
    )
    return (mixed, log_total)


def solution(mesh):
    in_specs = (
        P(("grp", "sp"), "tp"),
        P(),
        P("tp", None),
        P("tp", None),
        P(None, "tp"),
        P("tp"),
        P("tp", None),
        P("tp", None),
        P("tp", None),
        P("tp", ("grp", "sp")),
        P("tp", None),
        P("tp", None),
    )
    out_specs = (P(("grp", "sp", "tp"), None), P("tp", ("grp", "sp")))
    heads_here = HEADS // mesh.shape["tp"]
    fits = heads_here == mesh.shape["sp"] and mesh.shape["tp"] % 2 == 0
    body = functools.partial(fused_local, mesh.shape["sp"], mesh.shape["tp"]) if fits else local
    return jax.shard_map(body, mesh=mesh, in_specs=in_specs, out_specs=out_specs, check_vma=False)
```

```python
import functools
import jax
import jax.numpy as jnp
from jax import lax
from jax.experimental import pallas as pl
from jax.experimental.pallas import tpu as pltpu
from jax.sharding import PartitionSpec as P

D = 2048
CONV_CH = 1024
HEADS = 16


neg_large = -1e30


def passed_along(block, axis, distance):
    devices = range(lax.axis_size(axis))
    route = [(i - distance, i) for i in devices if i - distance in devices]
    return lax.ppermute(block, axis, route)


def block_terms(q_blk, q_cum, k_blk, v_blk, k_cum, q_first, k_first):
    score_scale = q_blk.shape[2] ** (-0.5)
    scores = (
        jnp.einsum("qhd,khd->hqk", q_blk, k_blk, preferred_element_type=jnp.float32) * score_scale
    )
    scores = scores + q_cum[:, :, None] - k_cum[:, None, :]
    q_pos = q_first + jnp.arange(q_blk.shape[0], dtype=jnp.int32)
    k_pos = k_first + jnp.arange(k_blk.shape[0], dtype=jnp.int32)
    allowed = k_pos[None, :] <= q_pos[:, None]
    scores = jnp.where(allowed[None], scores, -jnp.inf)
    block_top = jnp.max(scores, axis=-1)
    weights = jnp.exp(scores - block_top[..., None])
    block_total = jnp.sum(weights, axis=-1)
    block_out = jnp.einsum(
        "hqk,khd->hqd", weights.astype(jnp.bfloat16), v_blk, preferred_element_type=jnp.float32
    ).astype(jnp.bfloat16)
    return (block_top, block_total, block_out)


def merge_terms(state, terms):
    top_now, total_now, acc_now = state
    block_top, block_total, block_out = terms
    top_new = jnp.maximum(top_now, block_top)
    keep_old = jnp.exp(top_now - top_new)
    keep_new = jnp.exp(block_top - top_new)
    return (
        top_new,
        total_now * keep_old + block_total * keep_new,
        acc_now * keep_old[..., None] + block_out.astype(jnp.float32) * keep_new[..., None],
    )


def local(
    inputs,
    norm_gain,
    w_conv_in,
    w_conv_gate,
    conv_kernel,
    ln_gain,
    w_query,
    w_key,
    w_value,
    cum_gate,
    w_conv_out,
    w_attn_out,
):
    rows_here = inputs.shape[0]
    conv_width = w_conv_in.shape[0]
    attn_width = w_query.shape[0]
    heads_here = cum_gate.shape[0]
    head_dim = attn_width // heads_here
    taps_count = conv_kernel.shape[0]
    w_all = jnp.concatenate([w_conv_in, w_conv_gate, w_query, w_key, w_value], axis=0)
    gain_all = norm_gain.astype(jnp.float32)
    contract_dims = (((1,), (1,)), ((), ()))
    piece_f = lax.all_gather(inputs, "tp", axis=1, tiled=True).astype(jnp.float32)
    scaled_piece = (piece_f * gain_all[None, :]).astype(jnp.bfloat16)
    raw_proj = lax.dot_general(
        scaled_piece, w_all, contract_dims, preferred_element_type=jnp.float32
    )
    squares = jnp.sum(piece_f * piece_f, axis=1)
    rms = lax.rsqrt(squares / D + 1e-06)[:, None]
    proj = raw_proj * rms
    conv_in = proj[:, :conv_width]
    conv_gate = proj[:, conv_width : 2 * conv_width]
    query = proj[:, 2 * conv_width : 2 * conv_width + attn_width].astype(jnp.bfloat16)
    key_rows = proj[:, 2 * conv_width + attn_width : 2 * conv_width + 2 * attn_width].astype(
        jnp.bfloat16
    )
    value = proj[:, 2 * conv_width + 2 * attn_width :].astype(jnp.bfloat16)
    glu = (conv_in * jax.nn.sigmoid(conv_gate)).astype(jnp.bfloat16)
    rim_rows = passed_along(glu[rows_here - (taps_count - 1) :], "sp", 1)
    extended = jnp.concatenate([rim_rows, glu], axis=0)
    kernel = conv_kernel.astype(jnp.float32)
    conv_sum = jnp.zeros((rows_here, conv_width), jnp.float32)
    for tap_idx in range(taps_count):
        conv_sum = (
            conv_sum
            + extended[tap_idx : tap_idx + rows_here].astype(jnp.float32) * kernel[tap_idx][None, :]
        )
    chan_first, chan_second = lax.psum(
        (jnp.sum(conv_sum, axis=1), jnp.sum(conv_sum * conv_sum, axis=1)), "tp"
    )
    chan_mean = (chan_first / CONV_CH)[:, None]
    chan_var = (chan_second / CONV_CH)[:, None] - chan_mean * chan_mean
    normed = (
        (conv_sum - chan_mean) * lax.rsqrt(chan_var + 1e-05) * ln_gain.astype(jnp.float32)[None, :]
    )
    conv_out = jax.nn.silu(normed).astype(jnp.bfloat16)
    q_heads = query.reshape(rows_here, heads_here, head_dim)
    cum_all = lax.all_gather(cum_gate.T, "sp", axis=0, tiled=True)
    own_first = lax.axis_index("sp") * rows_here
    start_state = (
        jnp.full((heads_here, rows_here), neg_large, jnp.float32),
        jnp.zeros((heads_here, rows_here), jnp.float32),
        jnp.zeros((heads_here, rows_here, head_dim), jnp.float32),
    )
    state = start_state
    k_piece = lax.all_gather(key_rows, "sp", axis=0, tiled=True)
    v_piece = lax.all_gather(value, "sp", axis=0, tiled=True)
    block_count = k_piece.shape[0] // rows_here
    k_split = k_piece.reshape(block_count, rows_here, heads_here, head_dim)
    v_split = v_piece.reshape(block_count, rows_here, heads_here, head_dim)

    def visit(carry, item):
        k_blk, v_blk, block_idx = item
        k_first = block_idx * rows_here
        k_cum = lax.dynamic_slice_in_dim(cum_all, k_first, rows_here, 0).T

        def take_block(inner):
            return merge_terms(
                inner, block_terms(q_heads, cum_gate, k_blk, v_blk, k_cum, own_first, k_first)
            )

        def skip_block(inner):
            return inner

        return (lax.cond(k_first <= own_first, take_block, skip_block, carry), None)

    state, unused = lax.scan(
        visit, state, (k_split, v_split, jnp.arange(block_count, dtype=jnp.int32))
    )
    top_all, total_all, acc_all = state
    attn_out = (
        (acc_all / total_all[..., None])
        .transpose(1, 0, 2)
        .reshape(rows_here, attn_width)
        .astype(jnp.bfloat16)
    )
    log_total = top_all + jnp.log(total_all)
    mixed = lax.psum_scatter(
        (
            jnp.dot(conv_out, w_conv_out, preferred_element_type=jnp.float32)
            + jnp.dot(attn_out, w_attn_out, preferred_element_type=jnp.float32)
        ).astype(jnp.bfloat16),
        "tp",
        scatter_dimension=0,
        tiled=True,
    )
    return (mixed, log_total)


AG_CHUNKS = 8
OUT_CHUNKS = 4
MESH = pl.DeviceIdType.MESH
NT = (((1,), (1,)), ((), ()))


def fused_kernel(
    n_sp,
    n_tp,
    x_hbm,
    gain_ref,
    wci_hbm,
    wcg_hbm,
    ck_ref,
    lng_ref,
    wq_hbm,
    wk_hbm,
    wv_hbm,
    cum_ref,
    wco_hbm,
    wao_hbm,
    out_ref,
    log_ref,
    xg,
    xs,
    wbuf,
    wco,
    wao,
    acc,
    ss,
    zsend,
    zrecv,
    q_s,
    k_s,
    v_s,
    v_t,
    out_loc,
    lse_loc,
    cum_col,
    cum_recv,
    ext,
    halo_src,
    halo,
    csum,
    st_send,
    st_recv,
    cpart,
    ret_send,
    ret_recv,
    att_s,
    lse_send,
    lse_recv,
    d_send,
    d_recv,
    x_send,
    x_recv,
    parts,
    wsem,
    owsem,
    xsem,
    ag_send,
    ag_recv,
    zs_sem,
    zr_sem,
    cs_sem,
    cr_sem,
    hs_sem,
    hr_sem,
    ss_sem,
    sr_sem,
    rs_sem,
    rr_sem,
    ls_sem,
    lr_sem,
    ds_sem,
    dr_sem,
    xs_sem,
    xr_sem,
):
    f32, bf16 = jnp.float32, jnp.bfloat16
    z = lax.axis_index("sp")
    me = lax.axis_index("tp")
    chip, core = me // 2, me % 2
    chips = n_tp // 2
    rows, width = x_hbm.shape
    conv_w = wci_hbm.shape[0]
    attn_w = wq_hbm.shape[0]
    heads = n_sp
    hd = attn_w // heads
    d_all = wci_hbm.shape[1]
    partner = chip * 2 + 1 - core

    def remote(src, dst, s, r, dev):
        return pltpu.make_async_remote_copy(
            src_ref=src, dst_ref=dst, send_sem=s, recv_sem=r, device_id=dev, device_id_type=MESH
        )

    def same_core(dist):
        return lax.rem(chip + dist, chips) * 2 + core

    def other_core(dist):
        return lax.rem(chip + dist, chips) * 2 + 1 - core

    def piece_owner(rel):
        return same_core(rel // 2) if rel % 2 == 0 else other_core(rel // 2)

    def piece_source(rel):
        back = chips - rel // 2
        return same_core(back) if rel % 2 == 0 else other_core(back)

    barrier = pltpu.get_barrier_semaphore()
    for rel in range(1, n_tp):
        pl.semaphore_signal(
            barrier, inc=1, device_id={"tp": piece_owner(rel)}, device_id_type=MESH
        )
    for dist in range(1, n_sp):
        pl.semaphore_signal(
            barrier, inc=1, device_id={"sp": lax.rem(z + dist, n_sp)}, device_id_type=MESH
        )

    own_copy = pltpu.make_async_copy(x_hbm, xg.at[0], xsem)
    own_copy.start()
    loads = []
    for h in range(heads):
        loads.append((wk_hbm.at[pl.ds(h * hd, hd)], wbuf.at[pl.ds(2 * h * hd, hd)]))
        loads.append((wv_hbm.at[pl.ds(h * hd, hd)], wbuf.at[pl.ds((2 * h + 1) * hd, hd)]))
    loads.append((wq_hbm, wbuf.at[pl.ds(2 * attn_w, attn_w)]))
    qkv_loads = len(loads)
    qkv_w = 3 * attn_w
    loads.append((wci_hbm, wbuf.at[pl.ds(qkv_w, conv_w)]))
    loads.append((wcg_hbm, wbuf.at[pl.ds(qkv_w + conv_w, conv_w)]))
    wcopies = [pltpu.make_async_copy(a, b, wsem.at[i]) for i, (a, b) in enumerate(loads)]
    wco_copy = pltpu.make_async_copy(wco_hbm, wco, owsem.at[0])
    wao_copy = pltpu.make_async_copy(wao_hbm, wao, owsem.at[1])
    for c in wcopies:
        c.start()
    wco_copy.start()
    wao_copy.start()

    pl.semaphore_wait(barrier, n_tp - 1 + n_sp - 1)

    rc = rows // AG_CHUNKS

    def ag_copy(rel, kind, c):
        r = pl.ds(c * rc, rc)
        if kind == "own":
            return remote(
                x_hbm.at[r], xg.at[rel, r], ag_send.at[rel, c], ag_recv.at[rel, c],
                {"tp": piece_owner(rel)},
            )
        return remote(
            xg.at[rel - 1, r], xg.at[rel, r], ag_send.at[rel, c], ag_recv.at[rel, c],
            {"tp": partner},
        )

    order = [AG_CHUNKS - 1] + list(range(AG_CHUNKS - 1))
    ag = {}
    for c in order:
        for dist in range(1, chips):
            ag[2 * dist, c] = ag_copy(2 * dist, "own", c)
            ag[2 * dist, c].start()
    for c in order:
        ag[1, c] = ag_copy(1, "own", c)
        ag[1, c].start()
    cums = []
    for dist in range(1, n_sp):
        cp = remote(
            cum_ref, cum_recv.at[z], cs_sem.at[dist], cr_sem.at[dist],
            {"sp": lax.rem(z + dist, n_sp)},
        )
        cp.start()
        cums.append(cp)
    cum_recv[z] = cum_ref[...]

    def prepare(rel, c0, n):
        r = pl.ds(c0, n)
        owner = piece_source(rel)
        raw = xg[rel, r].astype(f32)
        g = gain_ref[pl.ds(pl.multiple_of(owner * width, width), width)].astype(f32).reshape(1, width)
        xs[rel, r] = (raw * g).astype(bf16)
        return jnp.sum(raw * raw, axis=1, keepdims=True)

    def wcols(rel, first, n):
        owner = piece_source(rel)
        return wbuf[pl.ds(first, n), pl.ds(pl.multiple_of(owner * width, width), width)]

    own_copy.wait()
    ss[...] = prepare(0, 0, rows)
    for c in wcopies[:qkv_loads]:
        c.wait()
    acc[:, :qkv_w] = lax.dot_general(xs[0], wcols(0, 0, qkv_w), NT, preferred_element_type=f32)
    for c in wcopies[qkv_loads:]:
        c.wait()
    acc[:, qkv_w:] = lax.dot_general(
        xs[0], wcols(0, qkv_w, 2 * conv_w), NT, preferred_element_type=f32
    )
    for c in range(AG_CHUNKS):
        ag[1, c].wait_recv()
    ss[...] += prepare(1, 0, rows)
    acc[...] += lax.dot_general(
        xs[1], wcols(1, 0, qkv_w + 2 * conv_w), NT, preferred_element_type=f32
    )

    half = rc // 2
    spans = (pl.ds(0, rc), pl.ds(rc, half))

    def z_copy(dist, c, part):
        to = lax.rem(z + dist, n_sp)
        return remote(
            zsend.at[to, c, spans[part]],
            zrecv.at[z, c, spans[part]],
            zs_sem.at[dist, c, part],
            zr_sem.at[dist, c, part],
            {"sp": to},
        )

    def z_arrival(dist, c, part):
        src = lax.rem(z + n_sp - dist, n_sp)
        return remote(
            zsend.at[src, c, spans[part]],
            zrecv.at[src, c, spans[part]],
            zs_sem.at[dist, c, part],
            zr_sem.at[dist, c, part],
            {"sp": src},
        )

    def finish_chunk(c):
        r = pl.ds(c * rc, rc)
        total = acc[r, :qkv_w]
        sq = ss[r]
        for dist in range(1, chips):
            ag[2 * dist + 1, c].wait_recv()
            sq = sq + prepare(2 * dist + 1, c * rc, rc)
            total = total + lax.dot_general(
                xs[2 * dist + 1, r],
                wcols(2 * dist + 1, 0, qkv_w),
                NT,
                preferred_element_type=f32,
            )
        rms = lax.rsqrt(sq / d_all + 1e-06)
        ss[r] = rms
        total = total * rms
        for h in range(heads):
            zsend[h, c, :rc] = total[:, 2 * h * hd : 2 * (h + 1) * hd].astype(bf16)
            q_h = total[:, 2 * attn_w + h * hd : 2 * attn_w + (h + 1) * hd]
            zsend[h, c, rc:] = jnp.concatenate([q_h[:half], q_h[half:]], axis=1).astype(bf16)
        for dist in range(n_sp - 1, 0, -1):

            @pl.when(z < n_sp - 1)
            def _():
                z_copy(dist, c, 0).start()

            @pl.when(z > 0)
            def _():
                z_copy(dist, c, 1).start()

        zrecv[z, c] = zsend[z, c]

    rim = halo.shape[0]
    halo_copy = remote(
        halo_src, halo, hs_sem, hr_sem, {"sp": lax.rem(z + 1, n_sp)}
    )

    def gated(r):
        pre = acc[r, qkv_w:]
        for rel in range(2, n_tp):
            pre = pre + lax.dot_general(
                xs[rel, r], wcols(rel, qkv_w, 2 * conv_w), NT, preferred_element_type=f32
            )
        pre = pre * ss[r]
        return (pre[:, :conv_w] * jax.nn.sigmoid(pre[:, conv_w:])).astype(bf16)

    for k, c in enumerate(order):
        r = pl.ds(c * rc, rc)
        for dist in range(1, chips):
            ag[2 * dist, c].wait_recv()
            ag[2 * dist + 1, c] = ag_copy(2 * dist + 1, "relay", c)
            ag[2 * dist + 1, c].start()
        for dist in range(1, chips):
            ss[r] += prepare(2 * dist, c * rc, rc)
            acc[r, :qkv_w] += lax.dot_general(
                xs[2 * dist, r], wcols(2 * dist, 0, qkv_w), NT, preferred_element_type=f32
            )
        if k == 0:
            finish_chunk(c)
        elif k == 1:
            halo_src[...] = gated(pl.ds(rows - rim, rim))

            @pl.when(z < n_sp - 1)
            def _():
                halo_copy.start()

        else:
            finish_chunk(order[k - 1])
    finish_chunk(order[-1])

    glu = gated(pl.ds(0, rows))
    taps = ck_ref.shape[0]
    ext[rim:, :] = glu.astype(f32)
    blk = 64

    def conv_block(b, carry):
        first = pl.multiple_of(b * blk, blk)
        block = ext[pl.ds(first, blk + rim), :]
        tot = jnp.zeros((blk, conv_w), f32)
        for j in range(taps):
            off = rim - (taps - 1) + j
            tot = tot + block[off : off + blk] * ck_ref[j : j + 1, :].astype(f32)
        csum[pl.ds(first, blk), :] = tot
        return carry

    lax.fori_loop(1, rows // blk, conv_block, 0)
    for cp in cums:
        cp.wait_recv()
    for src in range(n_sp):
        cum_col[pl.ds(src * rows, rows)] = jnp.broadcast_to(
            cum_recv[src, pl.ds(z, 1)], (128, rows)
        ).T

    @pl.when(z == 0)
    def _():
        halo[...] = jnp.zeros_like(halo)

    @pl.when(z > 0)
    def _():
        halo_copy.wait_recv()

    ext[:rim, :] = halo[...].astype(f32)
    conv_block(0, 0)
    cs = csum[...]
    first = jnp.sum(cs, axis=1, keepdims=True)
    second = jnp.sum(cs * cs, axis=1, keepdims=True)
    lane = lax.broadcasted_iota(jnp.int32, (rows, 128), 1)
    both = jnp.where(lane == 0, first, second)
    st_send[...] = both.T[: st_send.shape[0]]
    stats = []
    for rel in range(1, n_tp):
        cp = remote(
            st_send, st_recv.at[rel - 1], ss_sem.at[rel], sr_sem.at[rel], {"tp": piece_owner(rel)}
        )
        cp.start()
        stats.append(cp)
    scale = hd ** (-0.5)
    low = lax.broadcasted_iota(jnp.int32, (rc, 2 * hd), 1) < hd
    wide_k = -(-rows // 128)
    allowed = lax.broadcasted_iota(jnp.int32, (rows, rows), 0) <= lax.broadcasted_iota(
        jnp.int32, (rows, rows), 1
    )

    def take_keys(tile, r0):
        kv = tile.astype(f32)
        k_s[pl.ds(r0, rc)] = kv[:, :hd].astype(bf16)
        v_s[pl.ds(r0, rc)] = jnp.where(low, pltpu.roll(kv, hd, 1), 1.0).astype(bf16)

    def take_queries(tile, r0):
        qt = tile.astype(f32) * scale
        q_s[pl.ds(r0, half)] = qt[:, :hd].astype(bf16)
        q_s[pl.ds(r0 + half, half)] = qt[:, hd:].astype(bf16)

    def attend(q, k, vt, cum_k, causal):
        sc = lax.dot_general(k, q, NT, preferred_element_type=f32) - cum_k
        if causal:
            sc = jnp.where(allowed, sc, -jnp.inf)
        top = jnp.max(sc, axis=0, keepdims=True)
        p = jnp.exp(sc - top).astype(bf16)
        both = jnp.dot(vt, p, preferred_element_type=f32)
        tot = both[hd : hd + 1]
        return both[:hd] / tot, top + jnp.log(tot)

    for h in range(heads):
        for c in range(AG_CHUNKS):
            take_keys(zsend[h, c, :rc], h * rows + c * rc)
            take_queries(zsend[h, c, rc:], h * rows + c * rc)
    v_t[...] = v_s[...].T
    for h in range(heads):
        own = pl.ds(h * rows, rows)
        own_cum = cum_ref[pl.ds(h, 1), :]
        col = jnp.broadcast_to(own_cum, (128, rows)).T
        out_loc[pl.ds(h * hd, hd), :], lse = attend(
            q_s[own], k_s[own], v_t[:, h * rows : (h + 1) * rows],
            jnp.concatenate([col] * wide_k, axis=1), True,
        )
        lse_loc[pl.ds(h, 1), :] = lse + own_cum
    for dist in range(1, n_sp):
        src = lax.rem(z + n_sp - dist, n_sp)
        for c in range(AG_CHUNKS):

            @pl.when(src < n_sp - 1)
            def _():
                z_arrival(dist, c, 0).wait_recv()

            @pl.when(src > 0)
            def _():
                z_arrival(dist, c, 1).wait_recv()

    for s in range(n_sp):
        for c in range(AG_CHUNKS):
            if s < n_sp - 1:
                take_keys(zrecv[s, c, :rc], s * rows + c * rc)
            if s > 0:
                take_queries(zrecv[s, c, rc:], s * rows + c * rc)
    far_keys = (n_sp - 1) * rows
    v_t[:, :far_keys] = v_s[:far_keys].T
    for i in [1 + k // 2 if k % 2 == 0 else n_sp - 1 - k // 2 for k in range(n_sp - 1)]:
        keys = i * rows
        o, lse = attend(
            q_s[pl.ds(i * rows, rows)], k_s[:keys], v_t[:, :keys],
            jnp.concatenate([cum_col[:keys]] * wide_k, axis=1), False,
        )
        ret_send[i] = o.astype(bf16)
        lse_send[i] = jnp.broadcast_to(lse + cum_recv[i, pl.ds(z, 1)], (8, rows))

        @pl.when(z != i)
        def _():
            remote(
                ret_send.at[i], ret_recv.at[z], rs_sem.at[i], rr_sem.at[z], {"sp": i}
            ).start()
            remote(
                lse_send.at[i], lse_recv.at[z], ls_sem.at[i], lr_sem.at[z], {"sp": i}
            ).start()

        @pl.when(z == i)
        def _():
            ret_recv[i] = ret_send[i]
            lse_recv[i] = lse_send[i]

    tot = st_send[...]
    for rel in range(1, n_tp):
        stats[rel - 1].wait_recv()
        tot = tot + st_recv[rel - 1]
    wide = jnp.concatenate([tot] * (128 // tot.shape[0]), axis=0).T
    mean = wide[:, 0:1] / CONV_CH
    var = wide[:, 1:2] / CONV_CH - mean * mean
    normed = (csum[...] - mean) * lax.rsqrt(var + 1e-05) * lng_ref[...].astype(f32).reshape(1, conv_w)
    conv_out = (normed / (1.0 + jnp.exp(-normed))).astype(bf16)
    wco_copy.wait()
    cpart[...] = jnp.dot(conv_out, wco[...], preferred_element_type=f32)

    for h in range(n_sp):

        @pl.when((z != h) & (z > 0))
        def _():
            remote(
                ret_send.at[h], ret_recv.at[h], rs_sem.at[h], rr_sem.at[h], {"sp": h}
            ).wait_recv()
            remote(
                lse_send.at[h], lse_recv.at[h], ls_sem.at[h], lr_sem.at[h], {"sp": h}
            ).wait_recv()

    @pl.when(z == 0)
    def _():
        log_ref[...] = lse_loc[...]

    @pl.when(z > 0)
    def _():
        for h in range(heads):
            r = pl.ds(h * hd, hd)
            near, far = lse_loc[pl.ds(h, 1), :], lse_recv[h, 0:1, :]
            top = jnp.maximum(near, far)
            w_near, w_far = jnp.exp(near - top), jnp.exp(far - top)
            tot = w_near + w_far
            out_loc[r, :] = (out_loc[r, :] * w_near + ret_recv[h].astype(f32) * w_far) / tot
            log_ref[pl.ds(h, 1), :] = top + jnp.log(tot)

    att_s[...] = out_loc[...].T.astype(bf16)
    wao_copy.wait()
    own_rows = rows // n_tp
    cw = d_all // OUT_CHUNKS
    mine = pl.ds(pl.multiple_of(core * own_rows, own_rows), own_rows)
    theirs = pl.ds(pl.multiple_of((1 - core) * own_rows, own_rows), own_rows)
    d2d, xc = {}, {}

    def exchange(dist):
        to_chip = lax.rem(chip + dist, chips)
        r = pl.ds(pl.multiple_of(to_chip * 2 * own_rows, 2 * own_rows), 2 * own_rows)
        for n in range(OUT_CHUNKS):
            cols = slice(n * cw, (n + 1) * cw)
            parts[dist, n] = cpart[r, cols] + jnp.dot(
                att_s[r, :], wao[:, cols], preferred_element_type=f32
            )
            d_send[dist, n] = parts[dist, n, theirs].astype(bf16)
            d2d[dist, n] = remote(
                d_send.at[dist, n],
                d_recv.at[dist, n],
                ds_sem.at[dist, n],
                dr_sem.at[dist, n],
                {"tp": partner},
            )
            d2d[dist, n].start()

    def forward(dist):
        for n in range(OUT_CHUNKS):
            d2d[dist, n].wait_recv()
            x_send[dist - 1, n] = (
                parts[dist, n, mine] + d_recv[dist, n].astype(f32)
            ).astype(bf16)
            xc[dist, n] = remote(
                x_send.at[dist - 1, n],
                x_recv.at[dist - 1, n],
                xs_sem.at[dist - 1, n],
                xr_sem.at[dist - 1, n],
                {"tp": same_core(dist)},
            )
            xc[dist, n].start()

    for dist in range(1, chips):
        exchange(dist)
    for dist in range(1, chips):
        forward(dist)
    exchange(0)
    for n in range(OUT_CHUNKS):
        d2d[0, n].wait_recv()
    for n in range(OUT_CHUNKS):
        tot = parts[0, n, mine] + d_recv[0, n].astype(f32)
        for dist in range(1, chips):
            xc[dist, n].wait_recv()
            tot = tot + x_recv[dist - 1, n].astype(f32)
        out_ref[:, n * cw : (n + 1) * cw] = tot.astype(bf16)

    for cp in list(ag.values()) + cums + stats + list(d2d.values()) + list(xc.values()):
        cp.wait_send()

    @pl.when(z < n_sp - 1)
    def _():
        halo_copy.wait_send()

    for dist in range(1, n_sp):
        for c in range(AG_CHUNKS):

            @pl.when(z < n_sp - 1)
            def _():
                z_copy(dist, c, 0).wait_send()

            @pl.when(z > 0)
            def _():
                z_copy(dist, c, 1).wait_send()

    for i in range(1, n_sp):

        @pl.when(z != i)
        def _():
            remote(
                ret_send.at[i], ret_recv.at[z], rs_sem.at[i], rr_sem.at[z], {"sp": i}
            ).wait_send()
            remote(
                lse_send.at[i], lse_recv.at[z], ls_sem.at[i], lr_sem.at[z], {"sp": i}
            ).wait_send()


def fused_local(
    n_sp,
    n_tp,
    inputs,
    norm_gain,
    w_conv_in,
    w_conv_gate,
    conv_kernel,
    ln_gain,
    w_query,
    w_key,
    w_value,
    cum_gate,
    w_conv_out,
    w_attn_out,
):
    f32, bf16 = jnp.float32, jnp.bfloat16
    rows, width = inputs.shape
    conv_w, d_all = w_conv_in.shape
    attn_w = w_query.shape[0]
    heads = cum_gate.shape[0]
    hd = attn_w // heads
    chips = n_tp // 2
    own_rows = rows // n_tp
    rc = rows // AG_CHUNKS
    rim = -(-(conv_kernel.shape[0] - 1) // 16) * 16
    cw = d_all // OUT_CHUNKS
    all_w = 3 * attn_w + 2 * conv_w
    dma = pltpu.SemaphoreType.DMA
    scratch = [
        pltpu.VMEM((n_tp, rows, width), bf16),
        pltpu.VMEM((n_tp, rows, width), bf16),
        pltpu.VMEM((all_w, d_all), bf16),
        pltpu.VMEM((conv_w, d_all), bf16),
        pltpu.VMEM((attn_w, d_all), bf16),
        pltpu.VMEM((rows, all_w), f32),
        pltpu.VMEM((rows, 1), f32),
        pltpu.VMEM((n_sp, AG_CHUNKS, rc + rc // 2, 2 * hd), bf16),
        pltpu.VMEM((n_sp, AG_CHUNKS, rc + rc // 2, 2 * hd), bf16),
        pltpu.VMEM((n_sp * rows, hd), bf16),
        pltpu.VMEM((n_sp * rows, hd), bf16),
        pltpu.VMEM((n_sp * rows, 2 * hd), bf16),
        pltpu.VMEM((2 * hd, n_sp * rows), bf16),
        pltpu.VMEM((attn_w, rows), f32),
        pltpu.VMEM((heads, rows), f32),
        pltpu.VMEM((n_sp * rows, 128), f32),
        pltpu.VMEM((n_sp, heads, rows), f32),
        pltpu.VMEM((rows + rim, conv_w), f32),
        pltpu.VMEM((rim, conv_w), bf16),
        pltpu.VMEM((rim, conv_w), bf16),
        pltpu.VMEM((rows, conv_w), f32),
        pltpu.VMEM((8, rows), f32),
        pltpu.VMEM((n_tp - 1, 8, rows), f32),
        pltpu.VMEM((rows, d_all), f32),
        pltpu.VMEM((n_sp, hd, rows), bf16),
        pltpu.VMEM((n_sp, hd, rows), bf16),
        pltpu.VMEM((rows, attn_w), bf16),
        pltpu.VMEM((n_sp, 8, rows), f32),
        pltpu.VMEM((n_sp, 8, rows), f32),
        pltpu.VMEM((chips, OUT_CHUNKS, own_rows, cw), bf16),
        pltpu.VMEM((chips, OUT_CHUNKS, own_rows, cw), bf16),
        pltpu.VMEM((chips - 1, OUT_CHUNKS, own_rows, cw), bf16),
        pltpu.VMEM((chips - 1, OUT_CHUNKS, own_rows, cw), bf16),
        pltpu.VMEM((chips, OUT_CHUNKS, 2 * own_rows, cw), f32),
        dma((2 * heads + 3,)),
        dma((2,)),
        dma,
        dma((n_tp, AG_CHUNKS)),
        dma((n_tp, AG_CHUNKS)),
        dma((n_sp, AG_CHUNKS, 2)),
        dma((n_sp, AG_CHUNKS, 2)),
        dma((n_sp,)),
        dma((n_sp,)),
        dma,
        dma,
        dma((n_tp,)),
        dma((n_tp,)),
        dma((n_sp,)),
        dma((n_sp,)),
        dma((n_sp,)),
        dma((n_sp,)),
        dma((chips, OUT_CHUNKS)),
        dma((chips, OUT_CHUNKS)),
        dma((chips - 1, OUT_CHUNKS)),
        dma((chips - 1, OUT_CHUNKS)),
    ]
    far = pl.BlockSpec(memory_space=pl.ANY)
    near = pl.BlockSpec(memory_space=pltpu.VMEM)
    mixed, log_total = pl.pallas_call(
        functools.partial(fused_kernel, n_sp, n_tp),
        out_shape=(
            pltpu.VMEM((own_rows, d_all), bf16),
            pltpu.VMEM((heads, rows), f32),
        ),
        in_specs=[far, near, far, far, near, near, far, far, far, near, far, far],
        out_specs=(near, near),
        scratch_shapes=scratch,
        compiler_params=pltpu.CompilerParams(
            collective_id=0, has_side_effects=True, vmem_limit_bytes=60 * 1024 * 1024
        ),
    )(
        inputs,
        norm_gain,
        w_conv_in,
        w_conv_gate,
        conv_kernel,
        ln_gain,
        w_query,
        w_key,
        w_value,
        cum_gate,
        w_conv_out,
        w_attn_out,
    )
    return (mixed, log_total)


def solution(mesh):
    in_specs = (
        P(("grp", "sp"), "tp"),
        P(),
        P("tp", None),
        P("tp", None),
        P(None, "tp"),
        P("tp"),
        P("tp", None),
        P("tp", None),
        P("tp", None),
        P("tp", ("grp", "sp")),
        P("tp", None),
        P("tp", None),
    )
    out_specs = (P(("grp", "sp", "tp"), None), P("tp", ("grp", "sp")))
    heads_here = HEADS // mesh.shape["tp"]
    fits = heads_here == mesh.shape["sp"] and mesh.shape["tp"] % 2 == 0
    body = functools.partial(fused_local, mesh.shape["sp"], mesh.shape["tp"]) if fits else local
    return jax.shard_map(body, mesh=mesh, in_specs=in_specs, out_specs=out_specs, check_vma=False)
```

```python
import functools
import jax
import jax.numpy as jnp
from jax import lax
from jax.experimental import pallas as pl
from jax.experimental.pallas import tpu as pltpu
from jax.sharding import PartitionSpec as P

D = 2048
CONV_CH = 1024
HEADS = 16


neg_large = -1e30


def passed_along(block, axis, distance):
    devices = range(lax.axis_size(axis))
    route = [(i - distance, i) for i in devices if i - distance in devices]
    return lax.ppermute(block, axis, route)


def block_terms(q_blk, q_cum, k_blk, v_blk, k_cum, q_first, k_first):
    score_scale = q_blk.shape[2] ** (-0.5)
    scores = (
        jnp.einsum("qhd,khd->hqk", q_blk, k_blk, preferred_element_type=jnp.float32) * score_scale
    )
    scores = scores + q_cum[:, :, None] - k_cum[:, None, :]
    q_pos = q_first + jnp.arange(q_blk.shape[0], dtype=jnp.int32)
    k_pos = k_first + jnp.arange(k_blk.shape[0], dtype=jnp.int32)
    allowed = k_pos[None, :] <= q_pos[:, None]
    scores = jnp.where(allowed[None], scores, -jnp.inf)
    block_top = jnp.max(scores, axis=-1)
    weights = jnp.exp(scores - block_top[..., None])
    block_total = jnp.sum(weights, axis=-1)
    block_out = jnp.einsum(
        "hqk,khd->hqd", weights.astype(jnp.bfloat16), v_blk, preferred_element_type=jnp.float32
    ).astype(jnp.bfloat16)
    return (block_top, block_total, block_out)


def merge_terms(state, terms):
    top_now, total_now, acc_now = state
    block_top, block_total, block_out = terms
    top_new = jnp.maximum(top_now, block_top)
    keep_old = jnp.exp(top_now - top_new)
    keep_new = jnp.exp(block_top - top_new)
    return (
        top_new,
        total_now * keep_old + block_total * keep_new,
        acc_now * keep_old[..., None] + block_out.astype(jnp.float32) * keep_new[..., None],
    )


def local(
    inputs,
    norm_gain,
    w_conv_in,
    w_conv_gate,
    conv_kernel,
    ln_gain,
    w_query,
    w_key,
    w_value,
    cum_gate,
    w_conv_out,
    w_attn_out,
):
    rows_here = inputs.shape[0]
    conv_width = w_conv_in.shape[0]
    attn_width = w_query.shape[0]
    heads_here = cum_gate.shape[0]
    head_dim = attn_width // heads_here
    taps_count = conv_kernel.shape[0]
    w_all = jnp.concatenate([w_conv_in, w_conv_gate, w_query, w_key, w_value], axis=0)
    gain_all = norm_gain.astype(jnp.float32)
    contract_dims = (((1,), (1,)), ((), ()))
    piece_f = lax.all_gather(inputs, "tp", axis=1, tiled=True).astype(jnp.float32)
    scaled_piece = (piece_f * gain_all[None, :]).astype(jnp.bfloat16)
    raw_proj = lax.dot_general(
        scaled_piece, w_all, contract_dims, preferred_element_type=jnp.float32
    )
    squares = jnp.sum(piece_f * piece_f, axis=1)
    rms = lax.rsqrt(squares / D + 1e-06)[:, None]
    proj = raw_proj * rms
    conv_in = proj[:, :conv_width]
    conv_gate = proj[:, conv_width : 2 * conv_width]
    query = proj[:, 2 * conv_width : 2 * conv_width + attn_width].astype(jnp.bfloat16)
    key_rows = proj[:, 2 * conv_width + attn_width : 2 * conv_width + 2 * attn_width].astype(
        jnp.bfloat16
    )
    value = proj[:, 2 * conv_width + 2 * attn_width :].astype(jnp.bfloat16)
    glu = (conv_in * jax.nn.sigmoid(conv_gate)).astype(jnp.bfloat16)
    rim_rows = passed_along(glu[rows_here - (taps_count - 1) :], "sp", 1)
    extended = jnp.concatenate([rim_rows, glu], axis=0)
    kernel = conv_kernel.astype(jnp.float32)
    conv_sum = jnp.zeros((rows_here, conv_width), jnp.float32)
    for tap_idx in range(taps_count):
        conv_sum = (
            conv_sum
            + extended[tap_idx : tap_idx + rows_here].astype(jnp.float32) * kernel[tap_idx][None, :]
        )
    chan_first, chan_second = lax.psum(
        (jnp.sum(conv_sum, axis=1), jnp.sum(conv_sum * conv_sum, axis=1)), "tp"
    )
    chan_mean = (chan_first / CONV_CH)[:, None]
    chan_var = (chan_second / CONV_CH)[:, None] - chan_mean * chan_mean
    normed = (
        (conv_sum - chan_mean) * lax.rsqrt(chan_var + 1e-05) * ln_gain.astype(jnp.float32)[None, :]
    )
    conv_out = jax.nn.silu(normed).astype(jnp.bfloat16)
    q_heads = query.reshape(rows_here, heads_here, head_dim)
    cum_all = lax.all_gather(cum_gate.T, "sp", axis=0, tiled=True)
    own_first = lax.axis_index("sp") * rows_here
    start_state = (
        jnp.full((heads_here, rows_here), neg_large, jnp.float32),
        jnp.zeros((heads_here, rows_here), jnp.float32),
        jnp.zeros((heads_here, rows_here, head_dim), jnp.float32),
    )
    state = start_state
    k_piece = lax.all_gather(key_rows, "sp", axis=0, tiled=True)
    v_piece = lax.all_gather(value, "sp", axis=0, tiled=True)
    block_count = k_piece.shape[0] // rows_here
    k_split = k_piece.reshape(block_count, rows_here, heads_here, head_dim)
    v_split = v_piece.reshape(block_count, rows_here, heads_here, head_dim)

    def visit(carry, item):
        k_blk, v_blk, block_idx = item
        k_first = block_idx * rows_here
        k_cum = lax.dynamic_slice_in_dim(cum_all, k_first, rows_here, 0).T

        def take_block(inner):
            return merge_terms(
                inner, block_terms(q_heads, cum_gate, k_blk, v_blk, k_cum, own_first, k_first)
            )

        def skip_block(inner):
            return inner

        return (lax.cond(k_first <= own_first, take_block, skip_block, carry), None)

    state, unused = lax.scan(
        visit, state, (k_split, v_split, jnp.arange(block_count, dtype=jnp.int32))
    )
    top_all, total_all, acc_all = state
    attn_out = (
        (acc_all / total_all[..., None])
        .transpose(1, 0, 2)
        .reshape(rows_here, attn_width)
        .astype(jnp.bfloat16)
    )
    log_total = top_all + jnp.log(total_all)
    mixed = lax.psum_scatter(
        (
            jnp.dot(conv_out, w_conv_out, preferred_element_type=jnp.float32)
            + jnp.dot(attn_out, w_attn_out, preferred_element_type=jnp.float32)
        ).astype(jnp.bfloat16),
        "tp",
        scatter_dimension=0,
        tiled=True,
    )
    return (mixed, log_total)


AG_CHUNKS = 4
OUT_CHUNKS = 4
MESH = pl.DeviceIdType.MESH
NT = (((1,), (1,)), ((), ()))


def fused_kernel(
    n_sp,
    n_tp,
    x_hbm,
    gain_ref,
    wci_hbm,
    wcg_hbm,
    ck_ref,
    lng_ref,
    wq_hbm,
    wk_hbm,
    wv_hbm,
    cum_ref,
    wco_hbm,
    wao_hbm,
    out_ref,
    log_ref,
    xg,
    xs,
    wbuf,
    wco,
    wao,
    acc,
    ss,
    zsend,
    zrecv,
    q_s,
    k_s,
    v_s,
    v_t,
    out_loc,
    lse_loc,
    cum_col,
    cum_recv,
    ext,
    halo_src,
    halo,
    csum,
    st_send,
    st_recv,
    cpart,
    ret_send,
    ret_recv,
    att_s,
    lse_send,
    lse_recv,
    d_send,
    d_recv,
    x_send,
    x_recv,
    parts,
    wsem,
    owsem,
    xsem,
    ag_send,
    ag_recv,
    zs_sem,
    zr_sem,
    cs_sem,
    cr_sem,
    hs_sem,
    hr_sem,
    ss_sem,
    sr_sem,
    rs_sem,
    rr_sem,
    ls_sem,
    lr_sem,
    ds_sem,
    dr_sem,
    xs_sem,
    xr_sem,
):
    f32, bf16 = jnp.float32, jnp.bfloat16
    z = lax.axis_index("sp")
    me = lax.axis_index("tp")
    chip, core = me // 2, me % 2
    chips = n_tp // 2
    rows, width = x_hbm.shape
    conv_w = wci_hbm.shape[0]
    attn_w = wq_hbm.shape[0]
    heads = n_sp
    hd = attn_w // heads
    d_all = wci_hbm.shape[1]
    partner = chip * 2 + 1 - core

    def remote(src, dst, s, r, dev):
        return pltpu.make_async_remote_copy(
            src_ref=src, dst_ref=dst, send_sem=s, recv_sem=r, device_id=dev, device_id_type=MESH
        )

    def same_core(dist):
        return lax.rem(chip + dist, chips) * 2 + core

    def other_core(dist):
        return lax.rem(chip + dist, chips) * 2 + 1 - core

    def piece_owner(rel):
        return same_core(rel // 2) if rel % 2 == 0 else other_core(rel // 2)

    def piece_source(rel):
        back = chips - rel // 2
        return same_core(back) if rel % 2 == 0 else other_core(back)

    barrier = pltpu.get_barrier_semaphore()
    for rel in range(1, n_tp):
        pl.semaphore_signal(
            barrier, inc=1, device_id={"tp": piece_owner(rel)}, device_id_type=MESH
        )
    for dist in range(1, n_sp):
        pl.semaphore_signal(
            barrier, inc=1, device_id={"sp": lax.rem(z + dist, n_sp)}, device_id_type=MESH
        )

    own_copy = pltpu.make_async_copy(x_hbm, xg.at[0], xsem)
    own_copy.start()
    loads = []
    for h in range(heads):
        loads.append((wk_hbm.at[pl.ds(h * hd, hd)], wbuf.at[pl.ds(2 * h * hd, hd)]))
        loads.append((wv_hbm.at[pl.ds(h * hd, hd)], wbuf.at[pl.ds((2 * h + 1) * hd, hd)]))
    loads.append((wq_hbm, wbuf.at[pl.ds(2 * attn_w, attn_w)]))
    qkv_loads = len(loads)
    qkv_w = 3 * attn_w
    loads.append((wci_hbm, wbuf.at[pl.ds(qkv_w, conv_w)]))
    loads.append((wcg_hbm, wbuf.at[pl.ds(qkv_w + conv_w, conv_w)]))
    wcopies = [pltpu.make_async_copy(a, b, wsem.at[i]) for i, (a, b) in enumerate(loads)]
    wco_copy = pltpu.make_async_copy(wco_hbm, wco, owsem.at[0])
    wao_copy = pltpu.make_async_copy(wao_hbm, wao, owsem.at[1])
    for c in wcopies:
        c.start()
    wco_copy.start()
    wao_copy.start()

    pl.semaphore_wait(barrier, n_tp - 1 + n_sp - 1)

    rc = rows // AG_CHUNKS

    def ag_copy(rel, kind, c):
        r = pl.ds(c * rc, rc)
        if kind == "own":
            return remote(
                x_hbm.at[r], xg.at[rel, r], ag_send.at[rel, c], ag_recv.at[rel, c],
                {"tp": piece_owner(rel)},
            )
        return remote(
            xg.at[rel - 1, r], xg.at[rel, r], ag_send.at[rel, c], ag_recv.at[rel, c],
            {"tp": partner},
        )

    order = [AG_CHUNKS - 1] + list(range(AG_CHUNKS - 1))
    ag = {}
    for c in order:
        for dist in range(1, chips):
            ag[2 * dist, c] = ag_copy(2 * dist, "own", c)
            ag[2 * dist, c].start()
    for c in order:
        ag[1, c] = ag_copy(1, "own", c)
        ag[1, c].start()
    cums = []
    for dist in range(1, n_sp):
        cp = remote(
            cum_ref, cum_recv.at[z], cs_sem.at[dist], cr_sem.at[dist],
            {"sp": lax.rem(z + dist, n_sp)},
        )
        cp.start()
        cums.append(cp)
    cum_recv[z] = cum_ref[...]

    def prepare(rel, c0, n):
        r = pl.ds(c0, n)
        owner = piece_source(rel)
        raw = xg[rel, r].astype(f32)
        g = gain_ref[pl.ds(pl.multiple_of(owner * width, width), width)].astype(f32).reshape(1, width)
        xs[rel, r] = (raw * g).astype(bf16)
        return jnp.sum(raw * raw, axis=1, keepdims=True)

    def wcols(rel, first, n):
        owner = piece_source(rel)
        return wbuf[pl.ds(first, n), pl.ds(pl.multiple_of(owner * width, width), width)]

    own_copy.wait()
    ss[...] = prepare(0, 0, rows)
    for c in wcopies[:qkv_loads]:
        c.wait()
    acc[:, :qkv_w] = lax.dot_general(xs[0], wcols(0, 0, qkv_w), NT, preferred_element_type=f32)
    for c in wcopies[qkv_loads:]:
        c.wait()
    acc[:, qkv_w:] = lax.dot_general(
        xs[0], wcols(0, qkv_w, 2 * conv_w), NT, preferred_element_type=f32
    )
    for c in range(AG_CHUNKS):
        ag[1, c].wait_recv()
    ss[...] += prepare(1, 0, rows)
    acc[...] += lax.dot_general(
        xs[1], wcols(1, 0, qkv_w + 2 * conv_w), NT, preferred_element_type=f32
    )

    half = rc // 2
    spans = (pl.ds(0, rc), pl.ds(rc, half))

    def z_copy(dist, c, part):
        to = lax.rem(z + dist, n_sp)
        return remote(
            zsend.at[to, c, spans[part]],
            zrecv.at[z, c, spans[part]],
            zs_sem.at[dist, c, part],
            zr_sem.at[dist, c, part],
            {"sp": to},
        )

    def z_arrival(dist, c, part):
        src = lax.rem(z + n_sp - dist, n_sp)
        return remote(
            zsend.at[src, c, spans[part]],
            zrecv.at[src, c, spans[part]],
            zs_sem.at[dist, c, part],
            zr_sem.at[dist, c, part],
            {"sp": src},
        )

    def finish_chunk(c):
        r = pl.ds(c * rc, rc)
        total = acc[r, :qkv_w]
        sq = ss[r]
        for dist in range(1, chips):
            ag[2 * dist + 1, c].wait_recv()
            sq = sq + prepare(2 * dist + 1, c * rc, rc)
            total = total + lax.dot_general(
                xs[2 * dist + 1, r],
                wcols(2 * dist + 1, 0, qkv_w),
                NT,
                preferred_element_type=f32,
            )
        rms = lax.rsqrt(sq / d_all + 1e-06)
        ss[r] = rms
        total = total * rms
        for h in range(heads):
            zsend[h, c, :rc] = total[:, 2 * h * hd : 2 * (h + 1) * hd].astype(bf16)
            q_h = total[:, 2 * attn_w + h * hd : 2 * attn_w + (h + 1) * hd]
            zsend[h, c, rc:] = jnp.concatenate([q_h[:half], q_h[half:]], axis=1).astype(bf16)
        for dist in range(n_sp - 1, 0, -1):

            @pl.when(z < n_sp - 1)
            def _():
                z_copy(dist, c, 0).start()

            @pl.when(z > 0)
            def _():
                z_copy(dist, c, 1).start()

        zrecv[z, c] = zsend[z, c]

    rim = halo.shape[0]
    halo_copy = remote(
        halo_src, halo, hs_sem, hr_sem, {"sp": lax.rem(z + 1, n_sp)}
    )

    def gated(r):
        pre = acc[r, qkv_w:]
        for rel in range(2, n_tp):
            pre = pre + lax.dot_general(
                xs[rel, r], wcols(rel, qkv_w, 2 * conv_w), NT, preferred_element_type=f32
            )
        pre = pre * ss[r]
        return (pre[:, :conv_w] * jax.nn.sigmoid(pre[:, conv_w:])).astype(bf16)

    for k, c in enumerate(order):
        r = pl.ds(c * rc, rc)
        for dist in range(1, chips):
            ag[2 * dist, c].wait_recv()
            ag[2 * dist + 1, c] = ag_copy(2 * dist + 1, "relay", c)
            ag[2 * dist + 1, c].start()
        for dist in range(1, chips):
            ss[r] += prepare(2 * dist, c * rc, rc)
            acc[r, :qkv_w] += lax.dot_general(
                xs[2 * dist, r], wcols(2 * dist, 0, qkv_w), NT, preferred_element_type=f32
            )
        if k == 0:
            finish_chunk(c)
        elif k == 1:
            halo_src[...] = gated(pl.ds(rows - rim, rim))

            @pl.when(z < n_sp - 1)
            def _():
                halo_copy.start()

        else:
            finish_chunk(order[k - 1])
    finish_chunk(order[-1])

    glu = gated(pl.ds(0, rows))
    taps = ck_ref.shape[0]
    ext[rim:, :] = glu.astype(f32)
    blk = 64

    def conv_block(b, carry):
        first = pl.multiple_of(b * blk, blk)
        block = ext[pl.ds(first, blk + rim), :]
        tot = jnp.zeros((blk, conv_w), f32)
        for j in range(taps):
            off = rim - (taps - 1) + j
            tot = tot + block[off : off + blk] * ck_ref[j : j + 1, :].astype(f32)
        csum[pl.ds(first, blk), :] = tot
        return carry

    lax.fori_loop(1, rows // blk, conv_block, 0)
    for cp in cums:
        cp.wait_recv()
    for src in range(n_sp):
        cum_col[pl.ds(src * rows, rows)] = jnp.broadcast_to(
            cum_recv[src, pl.ds(z, 1)], (128, rows)
        ).T

    @pl.when(z == 0)
    def _():
        halo[...] = jnp.zeros_like(halo)

    @pl.when(z > 0)
    def _():
        halo_copy.wait_recv()

    ext[:rim, :] = halo[...].astype(f32)
    conv_block(0, 0)
    cs = csum[...]
    first = jnp.sum(cs, axis=1, keepdims=True)
    second = jnp.sum(cs * cs, axis=1, keepdims=True)
    lane = lax.broadcasted_iota(jnp.int32, (rows, 128), 1)
    both = jnp.where(lane == 0, first, second)
    st_send[...] = both.T[: st_send.shape[0]]
    stats = []
    for rel in range(1, n_tp):
        cp = remote(
            st_send, st_recv.at[rel - 1], ss_sem.at[rel], sr_sem.at[rel], {"tp": piece_owner(rel)}
        )
        cp.start()
        stats.append(cp)
    scale = hd ** (-0.5)
    low = lax.broadcasted_iota(jnp.int32, (rc, 2 * hd), 1) < hd
    wide_k = -(-rows // 128)
    allowed = lax.broadcasted_iota(jnp.int32, (rows, rows), 0) <= lax.broadcasted_iota(
        jnp.int32, (rows, rows), 1
    )

    def take_keys(tile, r0):
        kv = tile.astype(f32)
        k_s[pl.ds(r0, rc)] = kv[:, :hd].astype(bf16)
        v_s[pl.ds(r0, rc)] = jnp.where(low, pltpu.roll(kv, hd, 1), 1.0).astype(bf16)

    def take_queries(tile, r0):
        qt = tile.astype(f32) * scale
        q_s[pl.ds(r0, half)] = qt[:, :hd].astype(bf16)
        q_s[pl.ds(r0 + half, half)] = qt[:, hd:].astype(bf16)

    def attend(q, k, vt, cum_k, causal):
        sc = lax.dot_general(k, q, NT, preferred_element_type=f32) - cum_k
        if causal:
            sc = jnp.where(allowed, sc, -jnp.inf)
        top = jnp.max(sc, axis=0, keepdims=True)
        p = jnp.exp(sc - top).astype(bf16)
        both = jnp.dot(vt, p, preferred_element_type=f32)
        tot = both[hd : hd + 1]
        return both[:hd] / tot, top + jnp.log(tot)

    for h in range(heads):
        for c in range(AG_CHUNKS):
            take_keys(zsend[h, c, :rc], h * rows + c * rc)
            take_queries(zsend[h, c, rc:], h * rows + c * rc)
    v_t[...] = v_s[...].T
    for h in range(heads):
        own = pl.ds(h * rows, rows)
        own_cum = cum_ref[pl.ds(h, 1), :]
        col = jnp.broadcast_to(own_cum, (128, rows)).T
        out_loc[pl.ds(h * hd, hd), :], lse = attend(
            q_s[own], k_s[own], v_t[:, h * rows : (h + 1) * rows],
            jnp.concatenate([col] * wide_k, axis=1), True,
        )
        lse_loc[pl.ds(h, 1), :] = lse + own_cum
    for dist in range(1, n_sp):
        src = lax.rem(z + n_sp - dist, n_sp)
        for c in range(AG_CHUNKS):

            @pl.when(src < n_sp - 1)
            def _():
                z_arrival(dist, c, 0).wait_recv()

            @pl.when(src > 0)
            def _():
                z_arrival(dist, c, 1).wait_recv()

    for s in range(n_sp):
        for c in range(AG_CHUNKS):
            if s < n_sp - 1:
                take_keys(zrecv[s, c, :rc], s * rows + c * rc)
            if s > 0:
                take_queries(zrecv[s, c, rc:], s * rows + c * rc)
    far_keys = (n_sp - 1) * rows
    v_t[:, :far_keys] = v_s[:far_keys].T
    for i in [1 + k // 2 if k % 2 == 0 else n_sp - 1 - k // 2 for k in range(n_sp - 1)]:
        keys = i * rows
        o, lse = attend(
            q_s[pl.ds(i * rows, rows)], k_s[:keys], v_t[:, :keys],
            jnp.concatenate([cum_col[:keys]] * wide_k, axis=1), False,
        )
        ret_send[i] = o.astype(bf16)
        lse_send[i] = jnp.broadcast_to(lse + cum_recv[i, pl.ds(z, 1)], (8, rows))

        @pl.when(z != i)
        def _():
            remote(
                ret_send.at[i], ret_recv.at[z], rs_sem.at[i], rr_sem.at[z], {"sp": i}
            ).start()
            remote(
                lse_send.at[i], lse_recv.at[z], ls_sem.at[i], lr_sem.at[z], {"sp": i}
            ).start()

        @pl.when(z == i)
        def _():
            ret_recv[i] = ret_send[i]
            lse_recv[i] = lse_send[i]

    tot = st_send[...]
    for rel in range(1, n_tp):
        stats[rel - 1].wait_recv()
        tot = tot + st_recv[rel - 1]
    wide = jnp.concatenate([tot] * (128 // tot.shape[0]), axis=0).T
    mean = wide[:, 0:1] / CONV_CH
    var = wide[:, 1:2] / CONV_CH - mean * mean
    normed = (csum[...] - mean) * lax.rsqrt(var + 1e-05) * lng_ref[...].astype(f32).reshape(1, conv_w)
    conv_out = (normed / (1.0 + jnp.exp(-normed))).astype(bf16)
    wco_copy.wait()
    cpart[...] = jnp.dot(conv_out, wco[...], preferred_element_type=f32)

    for h in range(n_sp):

        @pl.when((z != h) & (z > 0))
        def _():
            remote(
                ret_send.at[h], ret_recv.at[h], rs_sem.at[h], rr_sem.at[h], {"sp": h}
            ).wait_recv()
            remote(
                lse_send.at[h], lse_recv.at[h], ls_sem.at[h], lr_sem.at[h], {"sp": h}
            ).wait_recv()

    @pl.when(z == 0)
    def _():
        log_ref[...] = lse_loc[...]

    @pl.when(z > 0)
    def _():
        for h in range(heads):
            r = pl.ds(h * hd, hd)
            near, far = lse_loc[pl.ds(h, 1), :], lse_recv[h, 0:1, :]
            top = jnp.maximum(near, far)
            w_near, w_far = jnp.exp(near - top), jnp.exp(far - top)
            tot = w_near + w_far
            out_loc[r, :] = (out_loc[r, :] * w_near + ret_recv[h].astype(f32) * w_far) / tot
            log_ref[pl.ds(h, 1), :] = top + jnp.log(tot)

    att_s[...] = out_loc[...].T.astype(bf16)
    wao_copy.wait()
    own_rows = rows // n_tp
    cw = d_all // OUT_CHUNKS
    mine = pl.ds(pl.multiple_of(core * own_rows, own_rows), own_rows)
    theirs = pl.ds(pl.multiple_of((1 - core) * own_rows, own_rows), own_rows)
    d2d, xc = {}, {}

    def exchange(dist):
        to_chip = lax.rem(chip + dist, chips)
        r = pl.ds(pl.multiple_of(to_chip * 2 * own_rows, 2 * own_rows), 2 * own_rows)
        for n in range(OUT_CHUNKS):
            cols = slice(n * cw, (n + 1) * cw)
            parts[dist, n] = cpart[r, cols] + jnp.dot(
                att_s[r, :], wao[:, cols], preferred_element_type=f32
            )
            d_send[dist, n] = parts[dist, n, theirs].astype(bf16)
            d2d[dist, n] = remote(
                d_send.at[dist, n],
                d_recv.at[dist, n],
                ds_sem.at[dist, n],
                dr_sem.at[dist, n],
                {"tp": partner},
            )
            d2d[dist, n].start()

    def forward(dist):
        for n in range(OUT_CHUNKS):
            d2d[dist, n].wait_recv()
            x_send[dist - 1, n] = (
                parts[dist, n, mine] + d_recv[dist, n].astype(f32)
            ).astype(bf16)
            xc[dist, n] = remote(
                x_send.at[dist - 1, n],
                x_recv.at[dist - 1, n],
                xs_sem.at[dist - 1, n],
                xr_sem.at[dist - 1, n],
                {"tp": same_core(dist)},
            )
            xc[dist, n].start()

    for dist in range(1, chips):
        exchange(dist)
    for dist in range(1, chips):
        forward(dist)
    exchange(0)
    for n in range(OUT_CHUNKS):
        d2d[0, n].wait_recv()
    for n in range(OUT_CHUNKS):
        tot = parts[0, n, mine] + d_recv[0, n].astype(f32)
        for dist in range(1, chips):
            xc[dist, n].wait_recv()
            tot = tot + x_recv[dist - 1, n].astype(f32)
        out_ref[:, n * cw : (n + 1) * cw] = tot.astype(bf16)

    for cp in list(ag.values()) + cums + stats + list(d2d.values()) + list(xc.values()):
        cp.wait_send()

    @pl.when(z < n_sp - 1)
    def _():
        halo_copy.wait_send()

    for dist in range(1, n_sp):
        for c in range(AG_CHUNKS):

            @pl.when(z < n_sp - 1)
            def _():
                z_copy(dist, c, 0).wait_send()

            @pl.when(z > 0)
            def _():
                z_copy(dist, c, 1).wait_send()

    for i in range(1, n_sp):

        @pl.when(z != i)
        def _():
            remote(
                ret_send.at[i], ret_recv.at[z], rs_sem.at[i], rr_sem.at[z], {"sp": i}
            ).wait_send()
            remote(
                lse_send.at[i], lse_recv.at[z], ls_sem.at[i], lr_sem.at[z], {"sp": i}
            ).wait_send()


def fused_local(
    n_sp,
    n_tp,
    inputs,
    norm_gain,
    w_conv_in,
    w_conv_gate,
    conv_kernel,
    ln_gain,
    w_query,
    w_key,
    w_value,
    cum_gate,
    w_conv_out,
    w_attn_out,
):
    f32, bf16 = jnp.float32, jnp.bfloat16
    rows, width = inputs.shape
    conv_w, d_all = w_conv_in.shape
    attn_w = w_query.shape[0]
    heads = cum_gate.shape[0]
    hd = attn_w // heads
    chips = n_tp // 2
    own_rows = rows // n_tp
    rc = rows // AG_CHUNKS
    rim = -(-(conv_kernel.shape[0] - 1) // 16) * 16
    cw = d_all // OUT_CHUNKS
    all_w = 3 * attn_w + 2 * conv_w
    dma = pltpu.SemaphoreType.DMA
    scratch = [
        pltpu.VMEM((n_tp, rows, width), bf16),
        pltpu.VMEM((n_tp, rows, width), bf16),
        pltpu.VMEM((all_w, d_all), bf16),
        pltpu.VMEM((conv_w, d_all), bf16),
        pltpu.VMEM((attn_w, d_all), bf16),
        pltpu.VMEM((rows, all_w), f32),
        pltpu.VMEM((rows, 1), f32),
        pltpu.VMEM((n_sp, AG_CHUNKS, rc + rc // 2, 2 * hd), bf16),
        pltpu.VMEM((n_sp, AG_CHUNKS, rc + rc // 2, 2 * hd), bf16),
        pltpu.VMEM((n_sp * rows, hd), bf16),
        pltpu.VMEM((n_sp * rows, hd), bf16),
        pltpu.VMEM((n_sp * rows, 2 * hd), bf16),
        pltpu.VMEM((2 * hd, n_sp * rows), bf16),
        pltpu.VMEM((attn_w, rows), f32),
        pltpu.VMEM((heads, rows), f32),
        pltpu.VMEM((n_sp * rows, 128), f32),
        pltpu.VMEM((n_sp, heads, rows), f32),
        pltpu.VMEM((rows + rim, conv_w), f32),
        pltpu.VMEM((rim, conv_w), bf16),
        pltpu.VMEM((rim, conv_w), bf16),
        pltpu.VMEM((rows, conv_w), f32),
        pltpu.VMEM((8, rows), f32),
        pltpu.VMEM((n_tp - 1, 8, rows), f32),
        pltpu.VMEM((rows, d_all), f32),
        pltpu.VMEM((n_sp, hd, rows), bf16),
        pltpu.VMEM((n_sp, hd, rows), bf16),
        pltpu.VMEM((rows, attn_w), bf16),
        pltpu.VMEM((n_sp, 8, rows), f32),
        pltpu.VMEM((n_sp, 8, rows), f32),
        pltpu.VMEM((chips, OUT_CHUNKS, own_rows, cw), bf16),
        pltpu.VMEM((chips, OUT_CHUNKS, own_rows, cw), bf16),
        pltpu.VMEM((chips - 1, OUT_CHUNKS, own_rows, cw), bf16),
        pltpu.VMEM((chips - 1, OUT_CHUNKS, own_rows, cw), bf16),
        pltpu.VMEM((chips, OUT_CHUNKS, 2 * own_rows, cw), f32),
        dma((2 * heads + 3,)),
        dma((2,)),
        dma,
        dma((n_tp, AG_CHUNKS)),
        dma((n_tp, AG_CHUNKS)),
        dma((n_sp, AG_CHUNKS, 2)),
        dma((n_sp, AG_CHUNKS, 2)),
        dma((n_sp,)),
        dma((n_sp,)),
        dma,
        dma,
        dma((n_tp,)),
        dma((n_tp,)),
        dma((n_sp,)),
        dma((n_sp,)),
        dma((n_sp,)),
        dma((n_sp,)),
        dma((chips, OUT_CHUNKS)),
        dma((chips, OUT_CHUNKS)),
        dma((chips - 1, OUT_CHUNKS)),
        dma((chips - 1, OUT_CHUNKS)),
    ]
    far = pl.BlockSpec(memory_space=pl.ANY)
    near = pl.BlockSpec(memory_space=pltpu.VMEM)
    mixed, log_total = pl.pallas_call(
        functools.partial(fused_kernel, n_sp, n_tp),
        out_shape=(
            pltpu.VMEM((own_rows, d_all), bf16),
            pltpu.VMEM((heads, rows), f32),
        ),
        in_specs=[far, near, far, far, near, near, far, far, far, near, far, far],
        out_specs=(near, near),
        scratch_shapes=scratch,
        compiler_params=pltpu.CompilerParams(
            collective_id=0, has_side_effects=True, vmem_limit_bytes=60 * 1024 * 1024
        ),
    )(
        inputs,
        norm_gain,
        w_conv_in,
        w_conv_gate,
        conv_kernel,
        ln_gain,
        w_query,
        w_key,
        w_value,
        cum_gate,
        w_conv_out,
        w_attn_out,
    )
    return (mixed, log_total)


def solution(mesh):
    in_specs = (
        P(("grp", "sp"), "tp"),
        P(),
        P("tp", None),
        P("tp", None),
        P(None, "tp"),
        P("tp"),
        P("tp", None),
        P("tp", None),
        P("tp", None),
        P("tp", ("grp", "sp")),
        P("tp", None),
        P("tp", None),
    )
    out_specs = (P(("grp", "sp", "tp"), None), P("tp", ("grp", "sp")))
    heads_here = HEADS // mesh.shape["tp"]
    fits = heads_here == mesh.shape["sp"] and mesh.shape["tp"] % 2 == 0
    body = functools.partial(fused_local, mesh.shape["sp"], mesh.shape["tp"]) if fits else local
    return jax.shard_map(body, mesh=mesh, in_specs=in_specs, out_specs=out_specs, check_vma=False)
```
